32 devices in a mesh: ep: 4 (over y, x), tp: 8 (over z, core).
Axes of the slice: x: 2, y: 2, z: 4, core: 2. Of those that a mesh axis runs over, the one named last changes fastest.
Arguments:
- tokens: bfloat16 [4096, 2048], P('ep', 'tp'), may hold values from -48 to 48
- pre_gain: bfloat16 [2048], P('tp'), may hold values from 0.099609375 to 1.8984375
- route_ids: int32 [4096, 2], P('ep'), may hold values from 0 to 3, all different within a row; in each aligned block of 1024 rows (0 to 1023, 1024 to 2047, ...) at most 576 rows name the same one
- route_weights: float32 [4096, 2], P('ep'), may hold values from 0.1 to 1
- gate_weight: bfloat16 [4, 2048, 7168], P('ep', None, 'tp'), may hold values from -0.125 to 0.125
- up_weight: bfloat16 [4, 2048, 7168], P('ep', None, 'tp'), may hold values from -0.125 to 0.125
- down_weight: bfloat16 [4, 7168, 2048], P('ep', 'tp')
- post_gain: bfloat16 [2048], P('tp'), may hold values from 0.099609375 to 1.8984375
Outputs:
- mixed: bfloat16 [4096, 2048], P('ep', 'tp')
The draws below stay inside these ranges and needn't reach their ends.
Inputs may be any that keep to these rules, and one draw needn't show every extreme that they name: `route_ids`: each row names 2 different experts; among the rows of one index of ep no expert is named more than 576 times, a bound that some block reaches.
All inputs are finite; a program needn't handle non-finite values.
Results may differ from the reference program's by a relative error of at most 0.02.
Values may be sent and summed in bfloat16 or wider, within the bound.
A program may use at most 128 MiB of HBM per device.

```python
import math
import jax
import jax.numpy as jnp
import numpy as np
from jax import lax

D = 2048
FF = 7168
TOP = 2
TOK_DEV = 1024
EXPERTS = 4
TOKENS = 4096
CAP = 576
N_EP = 4
N_TP = 8


def column_profile(key):
    position = jnp.arange(D, dtype=jnp.float32) / D
    return 0.5 * jnp.exp(math.log(4.0) * position) * jax.random.uniform(key, (D,), jnp.float32, 0.6, 1.4)


def draw_tokens(key, part):
    first, second, third = jax.random.split(jax.random.fold_in(key, 11), 3)
    columns = column_profile(second)
    base = jnp.clip(jax.random.normal(first, (TOKENS, D), jnp.float32), -5.0, 5.0)
    row_scale = jnp.exp(jax.random.uniform(third, (TOKENS, 1), jnp.float32, math.log(0.3), math.log(3.0)))
    return (base * row_scale * columns[None, :]).astype(jnp.bfloat16)


def draw_down_weight(key, part):
    first, second = jax.random.split(jax.random.fold_in(key, 23), 2)
    columns = column_profile(second)
    base = jnp.clip(jax.random.normal(first, (EXPERTS, FF, D), jnp.float32), -5.0, 5.0)
    return (base * FF ** (-0.5) * columns[None, None, :]).astype(jnp.bfloat16)


def block_scale(rng, shape, cuts, least, top_value):
    def one(axis_at, parts):
        heights = jax.random.uniform(jax.random.fold_in(jax.random.fold_in(rng, 6), axis_at), (parts,), jnp.float32, least / len(cuts), top_value / len(cuts))
        return jnp.repeat(jnp.exp(heights), shape[axis_at] // parts).reshape((-1,) + (1,) * (len(shape) - axis_at - 1))

    factor_of = one(*cuts[0])
    for cut in cuts[1:]:
        factor_of = factor_of * one(*cut)
    return factor_of


def routed_block(key, own, number, rows, amount, top, most, skew):
    sequence = jax.random.permutation(key, amount)
    crowded, ordinary = portions_of(amount, rows * top, most, skew, True), portions_of(amount, rows * top, most, skew, False)
    places = jnp.arange(amount)

    def named(lengths, rotation):
        used = int((lengths > 0).sum())
        fixed = max(1, used // 4)
        passed = fixed + (places - fixed + rotation * (used - fixed)) % max(1, amount - fixed)
        return jnp.zeros((amount,), jnp.int32).at[sequence[jnp.where(places < fixed, places, passed)]].set(jnp.asarray(lengths, jnp.int32))

    lengths = jnp.where(number % 4 == 0, named(crowded, number // 4), named(ordinary, number - number // 4 - 1))
    mixed = jax.random.permutation(jax.random.fold_in(own, 3), amount)
    donor, receiver = mixed[0:amount // 2 * 2:2], mixed[1:amount // 2 * 2:2]
    room = jnp.minimum(lengths[donor] - 1, most - lengths[receiver]) // 2
    room = jnp.where((donor == sequence[0]) | (receiver == sequence[0]) | (lengths[receiver] == 0), 0, jnp.maximum(room, 0))
    passed = jax.random.randint(jax.random.fold_in(own, 4), (amount // 2,), 0, 1 << 20) % (room + 1)
    lengths = lengths.at[donor].add(-passed).at[receiver].add(passed)
    labels = jnp.searchsorted(jnp.cumsum(lengths), jnp.arange(rows * top), side="right").astype(jnp.int32)
    table = labels.reshape(top, rows).T
    table = table[jax.random.permutation(jax.random.fold_in(own, 1), rows)]
    rotation = jax.random.randint(jax.random.fold_in(own, 2), (rows, 1), 0, top)
    return jnp.take_along_axis(table, (jnp.arange(top)[None, :] + rotation) % top, axis=1)


def portions_of(amount, total, most, skew, full):
    loads = [(1 << 20) // math.isqrt(rank ** skew) + 1 for rank in range(1, amount + 1)]
    largest = most if full else min(most, max(-(-total // amount), total * loads[0] // sum(loads)))
    least = 1 if total - largest >= amount - 1 else 0
    counts, spare = [largest] + [least] * (amount - 1), total - largest - least * (amount - 1)
    while spare > 0:
        free = [i for i in range(1, amount) if counts[i] < largest] or [i for i in range(1, amount) if counts[i] < most]
        pool, budget = sum([loads[i] for i in free]), spare
        for i in free:
            addition = min(most - counts[i], max(1, budget * loads[i] // pool), spare)
            counts[i] = counts[i] + addition
            spare = spare - addition
    return np.array(counts)


def noise(stream_key, shape, deviation, most, pieces=(), kind=jnp.bfloat16):
    array = deviation * jax.random.normal(stream_key, shape, jnp.float32)
    if pieces:
        array = array * block_scale(stream_key, shape, pieces, -0.22, 0.18)
    return jnp.clip(array, -most, most).astype(kind)


def setup_inputs(seed: int = 0) -> dict:
    keys = jax.random.split(jax.random.key(seed), 9)
    tokens = draw_tokens(jax.random.fold_in(keys[8], 71), 0)
    pre_gain = jnp.clip(1.0 + 0.18 * jax.random.normal(keys[1], (D,), jnp.float32), 0.099609375, 1.8984375).astype(jnp.bfloat16)
    route_ids_keys = jax.random.split(jax.random.fold_in(keys[2], 1), TOKENS // TOK_DEV)
    route_ids_turns = jax.random.permutation(jax.random.fold_in(keys[2], 3), TOKENS // TOK_DEV)
    route_ids = jax.vmap(lambda own, number: routed_block(jax.random.fold_in(keys[2], 2), own, number, TOK_DEV, EXPERTS, TOP, CAP, 2))(route_ids_keys, route_ids_turns).reshape((TOKENS, TOP))
    route_weights = jnp.clip(jnp.exp(math.log(1.0) - 2.3025851 * jax.random.uniform(keys[3], (TOKENS, TOP), jnp.float32) ** block_scale(keys[3], (TOKENS, TOP), ((0, 4),), -0.2, 0.2)), 0.1, 1.0)
    gate_weight = noise(keys[4], (EXPERTS, D, FF), D ** -0.5, 0.125, ((0, 4), (2, 8)))
    up_weight = noise(keys[5], (EXPERTS, D, FF), D ** -0.5, 0.125, ((0, 4), (2, 8)))
    down_weight = draw_down_weight(jax.random.fold_in(keys[8], 71), 0)
    post_gain = jnp.clip(1.0 + 0.18 * jax.random.normal(keys[7], (D,), jnp.float32), 0.099609375, 1.8984375).astype(jnp.bfloat16)
    return dict(tokens=tokens, pre_gain=pre_gain, route_ids=route_ids, route_weights=route_weights, gate_weight=gate_weight, up_weight=up_weight, down_weight=down_weight, post_gain=post_gain)


epsilon = 1e-06

def reference(tokens, pre_gain, route_ids, route_weights, gate_weight, up_weight, down_weight, post_gain):
    values = tokens.astype(jnp.float32)
    normed = (values * lax.rsqrt(lax.optimization_barrier(jnp.mean(values * values, axis=1, keepdims=True)) + epsilon) * pre_gain.astype(jnp.float32)).astype(jnp.bfloat16)
    tok_total = tokens.shape[0]
    rows_total = N_EP * CAP
    hidden_units = FF // N_TP
    flat_ids = route_ids.reshape(-1).astype(jnp.int32)
    onehot = (flat_ids[:, None] == jnp.arange(EXPERTS, dtype=jnp.int32)[None, :]).astype(jnp.int32)
    slot_rank = lax.optimization_barrier(jnp.sum((jnp.cumsum(onehot, axis=0) - 1) * onehot, axis=1)).astype(jnp.int32)
    padded = jnp.concatenate([normed, jnp.zeros((1, D), jnp.bfloat16)], axis=0)
    positions = jnp.arange(tok_total * TOP, dtype=jnp.int32)

    def one_expert(expert):
        target = jnp.where(flat_ids == expert, slot_rank, rows_total).astype(jnp.int32)
        slot_table = jnp.full((rows_total,), tok_total * TOP, jnp.int32).at[target].set(positions, mode='drop')
        routed = padded[slot_table // TOP]
        gate_act = jnp.dot(routed, gate_weight[expert], preferred_element_type=jnp.float32)
        up_act = jnp.dot(routed, up_weight[expert], preferred_element_type=jnp.float32)
        hidden = (jax.nn.silu(gate_act) * up_act).astype(jnp.bfloat16)
        partials = jnp.einsum('rjf,jfd->jrd', hidden.reshape(rows_total, N_TP, hidden_units).astype(jnp.float32), down_weight[expert].reshape(N_TP, hidden_units, D).astype(jnp.float32))
        partials = lax.optimization_barrier(partials.astype(jnp.bfloat16)).astype(jnp.float32)
        return lax.optimization_barrier(jnp.sum(partials, axis=0)).astype(jnp.bfloat16)
    results = lax.map(one_expert, jnp.arange(EXPERTS, dtype=jnp.int32))
    copies = results.reshape(EXPERTS * rows_total, D)[flat_ids * rows_total + slot_rank]
    copies = copies.astype(jnp.float32).reshape(tok_total, TOP, D)
    combined = lax.optimization_barrier(jnp.sum(copies * route_weights[:, :, None], axis=1))
    scaled = combined * lax.rsqrt(lax.optimization_barrier(jnp.mean(combined * combined, axis=1, keepdims=True)) + epsilon)
    return (scaled * post_gain.astype(jnp.float32)).astype(jnp.bfloat16)
```

```python
import functools

import jax
import jax.numpy as jnp
from jax import lax
from jax.experimental import pallas as pl
from jax.experimental.pallas import tpu as pltpu
from jax.sharding import PartitionSpec as P

epsilon = 1e-06
MESH = pl.DeviceIdType.MESH
DMA = pltpu.SemaphoreType.DMA
BF16 = jnp.bfloat16
F32 = jnp.float32
LANES = 128


def flip(a, m, size):
    total, bit = 0, 1
    while bit < size:
        total = total + (((a // bit) % 2 + (m // bit) % 2) % 2) * bit
        bit *= 2
    return total


def columns_of(values):
    rows = values.shape[0]
    if rows < LANES:
        values = jnp.concatenate([values, jnp.zeros((LANES - rows, LANES), values.dtype)], axis=0)
    return values.T


def fold(wide, nb):
    row = lax.broadcasted_iota(jnp.int32, (nb, LANES), 0)
    total = None
    for r in range(nb):
        part = jnp.broadcast_to(wide[:, r * LANES : (r + 1) * LANES], (nb, LANES))
        total = part if total is None else jnp.where(row == r, part, total)
    return total


def squares_of(v, nb):
    square = v * v
    high = square.astype(BF16)
    low = (square - high.astype(F32)).astype(BF16)
    ones = jnp.ones((nb, v.shape[1]), BF16)
    dims = (((1,), (1,)), ((), ()))
    wide = lax.dot_general(ones, high, dims, preferred_element_type=F32)
    wide += lax.dot_general(ones, low, dims, preferred_element_type=F32)
    return fold(wide, nb)


def layer_kernel(
    L, G, cap, tile,
    x_ref, pre_ref, post_ref, ids_ref, rw_ref, gate_ref, up_ref, down_ref, out_ref,
    zbuf, nbuf, obuf, piece, wbuf, acc, hbuf, dbuf, rbuf, rin, abuf, tbuf,
    stat, stat2, kbuf, kcol, wcol, scol,
    zs, zr, es, er, fs, ds, dr, ws, dl, dps, dpr, hs, hr, rs, rr, as_, ar, ys, yr, ss, sr, ts, tr,
):
    tok, cols = x_ref.shape
    nb = tok // LANES
    n = 2 * L
    units = gate_ref.shape[1]
    rows = G * cap
    far = G - 1
    me, g = lax.axis_index("tp"), lax.axis_index("ep")
    core, z = lax.rem(me, 2), me // 2
    partner = {"tp": me + 1 - 2 * core}
    inside = jnp.logical_and(z > 0, z < L - 1)
    inner = jnp.minimum(z, L - 1 - z)
    width = n * cols

    def order(s):
        near = jnp.where(s % 2 == 1, z - (s + 1) // 2, z + (s + 1) // 2)
        rest = jnp.where(2 * z > L - 1, z - (s - inner), z + (s - inner))
        return jnp.where(s <= 2 * inner, near, rest)

    def beside(b):
        return jnp.logical_or(b == z + 1, b == z - 1)

    def group_rows(e):
        return pl.ds(pl.multiple_of(e * cap, 16), cap)

    def remote(src, dst, send, recv, to):
        return pltpu.make_async_remote_copy(
            src_ref=src, dst_ref=dst, send_sem=send, recv_sem=recv, device_id=to, device_id_type=MESH
        )

    def at_z(to):
        return {"tp": to * 2 + core}

    def at_g(m):
        return {"ep": flip(g, m, G)}

    def w_load(s, i):
        ref = (gate_ref, up_ref)[i]
        depth = pl.ds(pl.multiple_of(order(s) * 2 * cols, LANES), 2 * cols)
        return pltpu.make_async_copy(ref.at[depth], wbuf.at[s % 2, i], ws.at[s % 2, i])

    def my_units(c):
        return pl.ds(pl.multiple_of(c * units, 16), units)

    def down_part(b, c):
        return down_ref.at[:, pl.ds(pl.multiple_of((b * 2 + c) * cols, LANES), cols)]

    def down_own(b):
        return pltpu.make_async_copy(down_part(b, core), dbuf.at[b, my_units(core)], dl.at[b])

    def down_push(b):
        return remote(
            down_part(b, 1 - core), dbuf.at[b, my_units(core)], dps.at[b], dpr.at[b], partner
        )

    def z_copy(b, side):
        return remote(zbuf.at[b], zbuf.at[b], zs.at[side, b], zr.at[b], at_z(z + 1 - 2 * side))

    def e_copy(b, m):
        return remote(
            obuf.at[b, m - 1], piece.at[core, b, group_rows(g)], es.at[b, m], er.at[b, m], at_g(m)
        )

    def f_copy(side):
        area = piece.at[core, z, group_rows(flip(g, far, G))]
        return remote(area, area, fs.at[side], er.at[z, far], at_z(z + 1 - 2 * side))

    def d_copy(b, m):
        area = piece.at[core, b, group_rows(flip(g, m, G))]
        return remote(area, area, ds.at[b, m], dr.at[b, m], partner)

    def h_copy(m):
        area = hbuf.at[core, group_rows(flip(g, m, G))]
        return remote(area, area, hs.at[m], hr.at[m], partner)

    def r_copy(b, m):
        return remote(
            obuf.at[b, m - 1], rbuf.at[b, group_rows(g)], rs.at[b, m], rr.at[b, m], at_g(m)
        )

    def a_copy(b, side):
        return remote(obuf.at[b, far - 1], abuf.at[side], as_.at[side], ar.at[side], at_z(z + 1 - 2 * side))

    def y_copy(b, side):
        to = z + 1 - 2 * side
        slot = jnp.where(jnp.logical_and(to == b, side == 1), L, b)
        return remote(zbuf.at[b], rin.at[slot], ys.at[b], yr.at[slot], at_z(to))

    def stat_copy(buf, send, recv, k):
        to = lax.rem(me + k, n)
        return remote(buf.at[me], buf.at[me], send.at[to], recv.at[me], {"tp": to})

    def stat_wait(buf, send, recv, k):
        of = lax.rem(me + n - k, n)
        remote(buf.at[of], buf.at[of], send.at[of], recv.at[of], {"tp": of}).wait_recv()

    barrier = pltpu.get_barrier_semaphore()
    for k in range(1, n):
        pl.semaphore_signal(barrier, inc=1, device_id={"tp": lax.rem(me + k, n)}, device_id_type=MESH)
    for m in range(1, G):
        pl.semaphore_signal(barrier, inc=1, device_id=at_g(m), device_id_type=MESH)
    for s in range(2):
        for i in range(2):
            w_load(s, i).start()

    @pl.loop(0, L)
    def _(b):
        down_own(b).start()

    zbuf[z] = x_ref[...]
    stat[me, 0:nb] = squares_of(x_ref[...].astype(F32), nb)
    for c in range(cols // LANES):
        stat[me, nb + c : nb + c + 1] = pre_ref[:, c * LANES : (c + 1) * LANES].astype(F32)

    pl.semaphore_wait(barrier, n + G - 2)
    for k in range(1, n):
        stat_copy(stat, ss, sr, k).start()
    pl.when(z < L - 1)(z_copy(z, 0).start)
    pl.when(z > 0)(z_copy(z, 1).start)

    ids, weights = ids_ref[...], rw_ref[...]
    top = ids.shape[0]
    id_rows = [fold(ids[t : t + 1], nb) for t in range(top)]
    weight_rows = [fold(weights[t : t + 1], nb) for t in range(top)]
    members, shares = [], []
    for e in range(G):
        named = [r == e for r in id_rows]
        members.append(sum(jnp.where(q, 1.0, 0.0) for q in named))
        shares.append(sum(jnp.where(q, w, 0.0) for q, w in zip(named, weight_rows)))
    member = jnp.concatenate(members, axis=0)
    small = member.astype(BF16)
    lane_a = lax.broadcasted_iota(jnp.int32, (LANES, LANES), 0)
    lane_b = lax.broadcasted_iota(jnp.int32, (LANES, LANES), 1)
    both = jnp.concatenate(
        [jnp.where(lane_a < lane_b, 1.0, 0.0).astype(BF16), jnp.ones((LANES, LANES), BF16)], axis=1
    )
    counted = jnp.dot(small, both, preferred_element_type=F32)
    row_a = lax.broadcasted_iota(jnp.int32, (G * nb, G * nb), 0)
    row_b = lax.broadcasted_iota(jnp.int32, (G * nb, G * nb), 1)
    ahead = jnp.where(jnp.logical_and(row_a // nb == row_b // nb, row_b < row_a), 1.0, 0.0).astype(BF16)
    rank = counted[:, :LANES] + jnp.dot(
        ahead, counted[:, LANES:].astype(BF16), preferred_element_type=F32
    )
    base = (lax.broadcasted_iota(jnp.int32, (G * nb, LANES), 0) // nb * cap).astype(F32)
    key = jnp.where(member > 0.5, rank + base, -1.0)
    kbuf[...] = key.astype(jnp.int32)
    kcol[...] = columns_of(key).astype(jnp.int32)
    wcol[...] = columns_of(jnp.concatenate(shares, axis=0))

    for e in range(G):
        wanted = lax.broadcasted_iota(jnp.int32, (cap, LANES), 0) + e * cap
        for r in range(nb):
            l, lane = r * LANES // cols, r * LANES % cols
            rbuf[l, e * cap : (e + 1) * cap, lane : lane + LANES] = jnp.where(
                kbuf[e * nb + r : e * nb + r + 1] == wanted, 1.0, 0.0
            ).astype(BF16)

    def row_scale(buf, send, recv):
        for k in range(1, n):
            stat_wait(buf, send, recv, k)
        total = buf[0, 0:nb]
        for k in range(1, n):
            total = total + buf[k, 0:nb]
        return columns_of(lax.rsqrt(total / width + epsilon))

    scol[...] = row_scale(stat, ss, sr)

    @pl.loop(0, L)
    def _(b):
        down_push(b).start()

    def take(s):
        b = order(s)
        z_copy(b, 0).wait_recv()
        pl.when(jnp.logical_and(b < z, z < L - 1))(z_copy(b, 0).start)
        pl.when(jnp.logical_and(b > z, z > 0))(z_copy(b, 1).start)

    def process(s):
        b = order(s)
        gain = jnp.concatenate(
            [stat[b * 2 + core, nb + c : nb + c + 1] for c in range(cols // LANES)], axis=1
        )
        for r in range(nb):
            at = slice(r * LANES, (r + 1) * LANES)
            nbuf[at] = (zbuf[b, at].astype(F32) * scol[:, r : r + 1] * gain).astype(BF16)

        @pl.loop(0, G)
        def _(j):
            m = G - 1 - j

            @pl.when(jnp.logical_not(jnp.logical_and(m == far, beside(b))))
            def _():
                at = group_rows(flip(g, m, G))
                chooser = jnp.concatenate([rbuf[l, at] for l in range(tok // cols)], axis=1)
                chosen = jnp.dot(chooser, nbuf[...], preferred_element_type=F32).astype(BF16)

                @pl.when(m > 0)
                def _():
                    obuf[b, m - 1] = chosen
                    e_copy(b, m).start()

                @pl.when(m == 0)
                def _():
                    piece[core, b, group_rows(g)] = chosen
                    d_copy(b, 0).start()

    def gate_up(b, slot, at):
        left = jnp.concatenate([piece[0, b, at], piece[1, b, at]], axis=1)
        return [jnp.dot(left, wbuf[slot, i], preferred_element_type=F32) for i in range(2)]

    def finish(s):
        b, slot = order(s), s % 2

        @pl.loop(1, G)
        def _(j):
            m = G - j
            e_copy(b, m).wait_recv()

            @pl.when(jnp.logical_and(m == far, b == z))
            def _():
                pl.when(z < L - 1)(f_copy(0).start)
                pl.when(z > 0)(f_copy(1).start)

            d_copy(b, m).start()

        @pl.loop(0, G)
        def _(m):
            d_copy(b, m).wait_recv()

        for i in range(2):
            w_load(s, i).wait()

        @pl.loop(0, rows // tile)
        def _(t):
            at = pl.ds(pl.multiple_of(t * tile, 16), tile)
            both = gate_up(b, slot, at)

            @pl.when(s == 0)
            def _():
                for i in range(2):
                    acc[i, at] = both[i]

            @pl.when(s > 0)
            def _():
                for i in range(2):
                    acc[i, at] += both[i]

        @pl.when(s + 2 < L)
        def _():
            for i in range(2):
                w_load(s + 2, i).start()

    process(0)

    @pl.loop(1, L)
    def _(s):
        pl.when(jnp.logical_or(jnp.logical_not(inside), s == 1))(lambda: take(s))
        process(s)
        pl.when(jnp.logical_and(inside, s + 1 < L))(lambda: take(s + 1))
        finish(s - 1)

    def project(i, m):
        b = order(L - 1 - i)
        at = group_rows(flip(g, m, G))
        if units % LANES == 0:
            left = jnp.concatenate([hbuf[0, at], hbuf[1, at]], axis=1)
            result = jnp.dot(left, dbuf[b], preferred_element_type=F32)
        else:
            result = jnp.dot(hbuf[0, at], dbuf[b, 0:units], preferred_element_type=F32)
            result += jnp.dot(hbuf[1, at], dbuf[b, units:], preferred_element_type=F32)

        @pl.when(m == 0)
        def _():
            rbuf[b, at] = result.astype(BF16)

        @pl.when(jnp.logical_and(m > 0, m < far))
        def _():
            e_copy(b, m).wait_send()
            obuf[b, m - 1] = result.astype(BF16)
            r_copy(b, m).start()

        @pl.when(m == far)
        def _():
            @pl.when(beside(b))
            def _():
                obuf[b, far - 1] = result.astype(BF16)
                pl.when(b > z)(a_copy(b, 0).start)
                pl.when(b < z)(a_copy(b, 1).start)

            @pl.when(jnp.logical_not(beside(b)))
            def _():
                e_copy(b, far).wait_send()

                @pl.when(b == z)
                def _():
                    tbuf[0:cap] = result

                    @pl.when(z > 0)
                    def _():
                        a_copy(b, 0).wait_recv()
                        tbuf[0:cap] += abuf[0].astype(F32)

                    @pl.when(z < L - 1)
                    def _():
                        a_copy(b, 1).wait_recv()
                        tbuf[0:cap] += abuf[1].astype(F32)

                    obuf[b, far - 1] = tbuf[0:cap].astype(BF16)

                @pl.when(b != z)
                def _():
                    obuf[b, far - 1] = result.astype(BF16)

                r_copy(b, far).start()

    def down_ready(b):
        down_own(b).wait()
        down_push(b).wait_recv()

    last = order(L - 1)
    for i in range(2):
        w_load(L - 1, i).wait()
    down_ready(last)

    @pl.loop(0, G + 1)
    def _(m):
        @pl.when(jnp.logical_and(m > 0, m < G))
        def _():
            e_copy(last, m).wait_recv()
            d_copy(last, m).start()

        @pl.when(m > 0)
        def _():
            h_copy(m - 1).wait_recv()
            project(0, m - 1)

        @pl.when(m < G)
        def _():
            d_copy(last, m).wait_recv()
            first = flip(g, m, G) * cap

            @pl.loop(0, cap // tile)
            def _(t):
                at = pl.ds(pl.multiple_of(first + t * tile, 16), tile)
                both = gate_up(last, (L - 1) % 2, at)
                gates = acc[0, at] + both[0]
                half = 0.5 * gates
                hbuf[core, at] = ((half + half * jnp.tanh(half)) * (acc[1, at] + both[1])).astype(BF16)

            h_copy(m).start()

    @pl.loop(1, L)
    def _(i):
        b = order(L - 1 - i)
        down_ready(b)

        @pl.loop(0, G)
        def _(j):
            project(i, jnp.where(i == L - 1, j, G - 1 - j))

    pl.when(z < L - 1)(z_copy(z, 0).wait_send)
    pl.when(z > 0)(z_copy(z, 1).wait_send)
    pl.when(z < L - 1)(f_copy(0).wait_send)
    pl.when(z > 0)(f_copy(1).wait_send)

    @pl.loop(0, L)
    def _(b):
        pl.when(jnp.logical_and(b < z, z < L - 1))(z_copy(b, 0).wait_send)
        pl.when(jnp.logical_and(b > z, z > 0))(z_copy(b, 1).wait_send)

        @pl.loop(0, G)
        def _(m):
            d_copy(b, m).wait_send()

        @pl.when(beside(b))
        def _():
            rbuf[b, group_rows(flip(g, far, G))] = jnp.zeros((cap, cols), BF16)

    per = rows // tok
    blocks = rows // cols

    def mix_place(k):
        return k // (L * per), (k // per) % L, (k % per) * tok

    for k in range(blocks):
        c, b, first = mix_place(k)
        lane = lax.broadcasted_iota(jnp.int32, (LANES, cols), 1) + k * cols
        for r in range(nb):
            value = jnp.zeros((LANES, cols), F32)
            for e in range(k * cols // cap, ((k + 1) * cols - 1) // cap + 1):
                q = e * nb + r
                value = jnp.where(kcol[:, q : q + 1] == lane, wcol[:, q : q + 1], value)
            piece[c, b, first + r * LANES : first + (r + 1) * LANES] = value.astype(BF16)

    step = min(256, tok)

    def combined(b, t):
        parts = []
        for k in range(blocks):
            c, l, first = mix_place(k)
            parts.append(piece[c, l, pl.ds(pl.multiple_of(first + t * step, 16), step)])
        return jnp.dot(jnp.concatenate(parts, axis=1), rbuf[b], preferred_element_type=F32)

    def arrived(b):
        @pl.loop(1, G)
        def _(m):
            @pl.when(jnp.logical_not(jnp.logical_and(m == far, beside(b))))
            def _():
                r_copy(b, m).wait_recv()

    @pl.loop(0, L - 1)
    def _(i):
        b = order(L - 1 - i)
        more = jnp.where(b > z, z, L - 1 - z) > 0
        arrived(b)

        @pl.when(more)
        def _():
            remote(zbuf.at[b], rin.at[b], ys.at[b], yr.at[b], at_z(b)).wait_recv()

        @pl.loop(0, tok // step)
        def _(t):
            at = pl.ds(pl.multiple_of(t * step, 16), step)
            value = combined(b, t)

            @pl.when(more)
            def _():
                zbuf[b, at] = (value + rin[b, at].astype(F32)).astype(BF16)

            @pl.when(jnp.logical_not(more))
            def _():
                zbuf[b, at] = value.astype(BF16)

        pl.when(b > z)(y_copy(b, 0).start)
        pl.when(b < z)(y_copy(b, 1).start)

    arrived(z)

    @pl.loop(0, tok // step)
    def _(t):
        at = pl.ds(pl.multiple_of(t * step, 16), step)
        tbuf[at] = combined(z, t)

    for side, slot in ((0, z), (1, L)):
        @pl.when(z > 0 if side == 0 else z < L - 1)
        def _():
            remote(zbuf.at[z], rin.at[slot], ys.at[z], yr.at[slot], partner).wait_recv()
            tbuf[...] += rin[slot].astype(F32)

    stat2[me] = squares_of(tbuf[...], nb)
    for k in range(1, n):
        stat_copy(stat2, ts, tr, k).start()
    post = post_ref[...].astype(F32)
    scol[...] = row_scale(stat2, ts, tr)
    for r in range(nb):
        at = slice(r * LANES, (r + 1) * LANES)
        out_ref[at] = (tbuf[at] * scol[:, r : r + 1] * post).astype(BF16)

    for k in range(1, n):
        stat_copy(stat, ss, sr, k).wait_send()
        stat_copy(stat2, ts, tr, k).wait_send()

    pl.when(z < L - 1)(a_copy(z + 1, 0).wait_send)
    pl.when(z > 0)(a_copy(z - 1, 1).wait_send)

    @pl.loop(0, L)
    def _(b):
        down_push(b).wait_send()
        pl.when(b > z)(y_copy(b, 0).wait_send)
        pl.when(b < z)(y_copy(b, 1).wait_send)

        @pl.loop(1, G)
        def _(m):
            @pl.when(jnp.logical_not(jnp.logical_and(m == far, beside(b))))
            def _():
                r_copy(b, m).wait_send()

    @pl.loop(0, G)
    def _(m):
        h_copy(m).wait_send()


def on_device(
    tokens, pre_gain, route_ids, route_weights, gate_weight, up_weight, down_weight, post_gain
):
    tok, cols = tokens.shape
    top = route_ids.shape[1]
    G = lax.axis_size("ep")
    n = lax.axis_size("tp")
    L = n // 2
    cap = 9 * tok * top // (8 * G)
    rows = G * cap
    units = gate_weight.shape[2]
    nb = tok // LANES
    tile = cap
    vmem = pl.BlockSpec(memory_space=pltpu.VMEM)
    hbm = pl.BlockSpec(memory_space=pl.ANY)
    return pl.pallas_call(
        functools.partial(layer_kernel, L, G, cap, tile),
        out_shape=jax.ShapeDtypeStruct((tok, cols), BF16),
        in_specs=[vmem] * 5 + [hbm] * 3,
        out_specs=vmem,
        scratch_shapes=[
            pltpu.VMEM((L, tok, cols), BF16),
            pltpu.VMEM((tok, cols), BF16),
            pltpu.VMEM((L, G - 1, cap, cols), BF16),
            pltpu.VMEM((2, L, rows, cols), BF16),
            pltpu.VMEM((2, 2, 2 * cols, units), BF16),
            pltpu.VMEM((2, rows, units), F32),
            pltpu.VMEM((2, rows, units), BF16),
            pltpu.VMEM((L, 2 * units, cols), BF16),
            pltpu.VMEM((L, rows, cols), BF16),
            pltpu.VMEM((L + 1, tok, cols), BF16),
            pltpu.VMEM((2, cap, cols), BF16),
            pltpu.VMEM((tok, cols), F32),
            pltpu.VMEM((n, 2 * nb, LANES), F32),
            pltpu.VMEM((n, nb, LANES), F32),
            pltpu.VMEM((G * nb, LANES), jnp.int32),
            pltpu.VMEM((LANES, LANES), jnp.int32),
            pltpu.VMEM((LANES, LANES), F32),
            pltpu.VMEM((LANES, LANES), F32),
            DMA((2, L)), DMA((L,)),
            DMA((L, G)), DMA((L, G)),
            DMA((2,)),
            DMA((L, G)), DMA((L, G)),
            DMA((2, 2)),
            DMA((L,)), DMA((L,)), DMA((L,)),
            DMA((G,)), DMA((G,)),
            DMA((L, G)), DMA((L, G)),
            DMA((2,)), DMA((2,)),
            DMA((L,)), DMA((L + 1,)),
            DMA((n,)), DMA((n,)),
            DMA((n,)), DMA((n,)),
        ],
        compiler_params=pltpu.CompilerParams(
            collective_id=1, has_side_effects=True, vmem_limit_bytes=62 * 2**20
        ),
        name="layer",
    )(
        tokens, pre_gain.reshape(1, cols), post_gain.reshape(1, cols), route_ids.T, route_weights.T,
        gate_weight[0], up_weight[0], down_weight[0],
    )


def solution(mesh):
    placed = (
        P("ep", "tp"),
        P("tp"),
        P("ep", None),
        P("ep", None),
        P("ep", None, "tp"),
        P("ep", None, "tp"),
        P("ep", "tp", None),
        P("tp"),
    )
    return jax.shard_map(
        on_device, mesh=mesh, in_specs=placed, out_specs=P("ep", "tp"), check_vma=False
    )
```

```python
import functools

import jax
import jax.numpy as jnp
from jax import lax
from jax.experimental import pallas as pl
from jax.experimental.pallas import tpu as pltpu
from jax.sharding import PartitionSpec as P

epsilon = 1e-06
MESH = pl.DeviceIdType.MESH
DMA = pltpu.SemaphoreType.DMA
BF16 = jnp.bfloat16
F32 = jnp.float32
LANES = 128


def flip(a, m, size):
    total, bit = 0, 1
    while bit < size:
        total = total + (((a // bit) % 2 + (m // bit) % 2) % 2) * bit
        bit *= 2
    return total


def columns_of(values):
    rows = values.shape[0]
    if rows < LANES:
        values = jnp.concatenate([values, jnp.zeros((LANES - rows, LANES), values.dtype)], axis=0)
    return values.T


def fold(wide, nb):
    row = lax.broadcasted_iota(jnp.int32, (nb, LANES), 0)
    total = None
    for r in range(nb):
        part = jnp.broadcast_to(wide[:, r * LANES : (r + 1) * LANES], (nb, LANES))
        total = part if total is None else jnp.where(row == r, part, total)
    return total


def squares_of(v, nb):
    square = v * v
    high = square.astype(BF16)
    low = (square - high.astype(F32)).astype(BF16)
    ones = jnp.ones((nb, v.shape[1]), BF16)
    dims = (((1,), (1,)), ((), ()))
    wide = lax.dot_general(ones, high, dims, preferred_element_type=F32)
    wide += lax.dot_general(ones, low, dims, preferred_element_type=F32)
    return fold(wide, nb)


def layer_kernel(
    L, G, cap, tile,
    x_ref, pre_ref, post_ref, ids_ref, rw_ref, gate_ref, up_ref, down_ref, out_ref,
    zbuf, nbuf, obuf, piece, wbuf, acc, hbuf, dbuf, rbuf, rin, abuf, tbuf,
    stat, stat2, kbuf, kcol, wcol, scol,
    zs, zr, es, er, fs, ds, dr, ws, dl, dps, dpr, hs, hr, rs, rr, as_, ar, ys, yr, ss, sr, ts, tr, xs,
):
    tok, cols = nbuf.shape
    nb = tok // LANES
    n = 2 * L
    units = gate_ref.shape[1]
    rows = G * cap
    far = G - 1
    me, g = lax.axis_index("tp"), lax.axis_index("ep")
    core, z = lax.rem(me, 2), me // 2
    partner = {"tp": me + 1 - 2 * core}
    inside = jnp.logical_and(z > 0, z < L - 1)
    inner = jnp.minimum(z, L - 1 - z)
    width = n * cols

    def order(s):
        near = jnp.where(s % 2 == 1, z - (s + 1) // 2, z + (s + 1) // 2)
        rest = jnp.where(2 * z > L - 1, z - (s - inner), z + (s - inner))
        return jnp.where(s <= 2 * inner, near, rest)

    farthest = jnp.where(2 * z > L - 1, 0, L - 1)
    end_left = z == 1
    next_to_end = jnp.logical_or(z == 1, z == L - 2)

    def skipped(b):
        beside = jnp.logical_or(b == z + 1, b == z - 1)
        return jnp.where(inside, beside, b == farthest)

    def group_rows(e):
        return pl.ds(pl.multiple_of(e * cap, 16), cap)

    def remote(src, dst, send, recv, to):
        return pltpu.make_async_remote_copy(
            src_ref=src, dst_ref=dst, send_sem=send, recv_sem=recv, device_id=to, device_id_type=MESH
        )

    def at_z(to):
        return {"tp": to * 2 + core}

    def at_g(m):
        return {"ep": flip(g, m, G)}

    def w_load(s, i):
        ref = (gate_ref, up_ref)[i]
        depth = pl.ds(pl.multiple_of(order(s) * 2 * cols, LANES), 2 * cols)
        return pltpu.make_async_copy(ref.at[depth], wbuf.at[s % 2, i], ws.at[s % 2, i])

    def my_units(c):
        return pl.ds(pl.multiple_of(c * units, 16), units)

    def down_part(b, c):
        return down_ref.at[:, pl.ds(pl.multiple_of((b * 2 + c) * cols, LANES), cols)]

    def down_own(b):
        return pltpu.make_async_copy(down_part(b, core), dbuf.at[b, my_units(core)], dl.at[b])

    def down_push(b):
        return remote(
            down_part(b, 1 - core), dbuf.at[b, my_units(core)], dps.at[b], dpr.at[b], partner
        )

    def z_copy(b, side):
        return remote(zbuf.at[b], zbuf.at[b], zs.at[side, b], zr.at[b], at_z(z + 1 - 2 * side))

    def e_copy(b, m):
        return remote(
            obuf.at[b, m - 1], piece.at[core, b, group_rows(g)], es.at[b, m], er.at[b, m], at_g(m)
        )

    def f_copy(side):
        area = piece.at[core, z, group_rows(flip(g, far, G))]
        return remote(area, area, fs.at[side], er.at[z, far], at_z(z + 1 - 2 * side))

    def l_copy():
        area = piece.at[core, farthest, group_rows(flip(g, far, G))]
        return remote(area, area, fs.at[2], er.at[farthest, far], at_z(jnp.where(end_left, 0, L - 1)))

    def d_copy(b, m):
        area = piece.at[core, b, group_rows(flip(g, m, G))]
        return remote(area, area, ds.at[b, m], dr.at[b, m], partner)

    def h_copy(m):
        area = hbuf.at[core, group_rows(flip(g, m, G))]
        return remote(area, area, hs.at[m], hr.at[m], partner)

    def r_copy(b, m):
        return remote(
            obuf.at[b, m - 1], rbuf.at[b, group_rows(g)], rs.at[b, m], rr.at[b, m], at_g(m)
        )

    def a_copy(b, side):
        return remote(obuf.at[b, far - 1], abuf.at[side], as_.at[side], ar.at[side], at_z(z + 1 - 2 * side))

    def y_copy(b, side):
        to = z + 1 - 2 * side
        slot = jnp.where(jnp.logical_and(to == b, side == 1), L, b)
        return remote(zbuf.at[b], rin.at[slot], ys.at[b], yr.at[slot], at_z(to))

    def stat_copy(buf, send, recv, k):
        to = lax.rem(me + k, n)
        return remote(buf.at[me], buf.at[me], send.at[to], recv.at[me], {"tp": to})

    def stat_wait(buf, send, recv, k):
        of = lax.rem(me + n - k, n)
        remote(buf.at[of], buf.at[of], send.at[of], recv.at[of], {"tp": of}).wait_recv()

    barrier = pltpu.get_barrier_semaphore()
    for k in range(1, n):
        pl.semaphore_signal(barrier, inc=1, device_id={"tp": lax.rem(me + k, n)}, device_id_type=MESH)
    for m in range(1, G):
        pl.semaphore_signal(barrier, inc=1, device_id=at_g(m), device_id_type=MESH)
    x_load = pltpu.make_async_copy(x_ref, zbuf.at[z], xs.at[0])
    x_load.start()
    for s in range(2):
        for i in range(2):
            w_load(s, i).start()

    @pl.loop(0, L)
    def _(b):
        down_own(b).start()

    x_load.wait()
    stat[me, 0:nb] = squares_of(zbuf[z].astype(F32), nb)
    pre = pre_ref[...].astype(F32).reshape(1, cols)
    for c in range(cols // LANES):
        stat[me, nb + c : nb + c + 1] = pre[:, c * LANES : (c + 1) * LANES]

    pl.semaphore_wait(barrier, n + G - 2)
    for k in range(1, n):
        stat_copy(stat, ss, sr, k).start()
    pl.when(z < L - 1)(z_copy(z, 0).start)
    pl.when(z > 0)(z_copy(z, 1).start)

    ids, weights = ids_ref[...], rw_ref[...]
    top = ids.shape[0]
    id_rows = [fold(ids[t : t + 1], nb) for t in range(top)]
    weight_rows = [fold(weights[t : t + 1], nb) for t in range(top)]
    members, shares = [], []
    for e in range(G):
        named = [r == e for r in id_rows]
        members.append(sum(jnp.where(q, 1.0, 0.0) for q in named))
        shares.append(sum(jnp.where(q, w, 0.0) for q, w in zip(named, weight_rows)))
    member = jnp.concatenate(members, axis=0)
    small = member.astype(BF16)
    lane_a = lax.broadcasted_iota(jnp.int32, (LANES, LANES), 0)
    lane_b = lax.broadcasted_iota(jnp.int32, (LANES, LANES), 1)
    both = jnp.concatenate(
        [jnp.where(lane_a < lane_b, 1.0, 0.0).astype(BF16), jnp.ones((LANES, LANES), BF16)], axis=1
    )
    counted = jnp.dot(small, both, preferred_element_type=F32)
    row_a = lax.broadcasted_iota(jnp.int32, (G * nb, G * nb), 0)
    row_b = lax.broadcasted_iota(jnp.int32, (G * nb, G * nb), 1)
    ahead = jnp.where(jnp.logical_and(row_a // nb == row_b // nb, row_b < row_a), 1.0, 0.0).astype(BF16)
    rank = counted[:, :LANES] + jnp.dot(
        ahead, counted[:, LANES:].astype(BF16), preferred_element_type=F32
    )
    base = (lax.broadcasted_iota(jnp.int32, (G * nb, LANES), 0) // nb * cap).astype(F32)
    key = jnp.where(member > 0.5, rank + base, -1.0)
    kbuf[...] = key.astype(jnp.int32)
    kcol[...] = columns_of(key).astype(jnp.int32)
    wcol[...] = columns_of(jnp.concatenate(shares, axis=0))

    for e in range(G):
        wanted = lax.broadcasted_iota(jnp.int32, (cap, LANES), 0) + e * cap
        for r in range(nb):
            l, lane = r * LANES // cols, r * LANES % cols
            rbuf[l, e * cap : (e + 1) * cap, lane : lane + LANES] = jnp.where(
                kbuf[e * nb + r : e * nb + r + 1] == wanted, 1.0, 0.0
            ).astype(BF16)

    def row_scale(buf, send, recv):
        for k in range(1, n):
            stat_wait(buf, send, recv, k)
        total = buf[0, 0:nb]
        for k in range(1, n):
            total = total + buf[k, 0:nb]
        return columns_of(lax.rsqrt(total / width + epsilon))

    scol[...] = row_scale(stat, ss, sr)

    @pl.loop(0, L)
    def _(b):
        down_push(b).start()

    def take(s):
        b = order(s)
        z_copy(b, 0).wait_recv()
        pl.when(jnp.logical_and(b < z, z < L - 1))(z_copy(b, 0).start)
        pl.when(jnp.logical_and(b > z, z > 0))(z_copy(b, 1).start)

    def process(s):
        b = order(s)
        gain = jnp.concatenate(
            [stat[b * 2 + core, nb + c : nb + c + 1] for c in range(cols // LANES)], axis=1
        )
        for r in range(nb):
            at = slice(r * LANES, (r + 1) * LANES)
            nbuf[at] = (zbuf[b, at].astype(F32) * scol[:, r : r + 1] * gain).astype(BF16)

        @pl.loop(0, G)
        def _(j):
            m = G - 1 - j

            @pl.when(jnp.logical_not(jnp.logical_and(m == far, skipped(b))))
            def _():
                at = group_rows(flip(g, m, G))
                chooser = jnp.concatenate([rbuf[l, at] for l in range(tok // cols)], axis=1)
                chosen = jnp.dot(chooser, nbuf[...], preferred_element_type=F32).astype(BF16)

                @pl.when(m > 0)
                def _():
                    obuf[b, m - 1] = chosen
                    e_copy(b, m).start()

                @pl.when(m == 0)
                def _():
                    piece[core, b, group_rows(g)] = chosen
                    d_copy(b, 0).start()

    def gate_up(b, slot, at):
        left = jnp.concatenate([piece[0, b, at], piece[1, b, at]], axis=1)
        return [jnp.dot(left, wbuf[slot, i], preferred_element_type=F32) for i in range(2)]

    def finish(s):
        b, slot = order(s), s % 2

        @pl.loop(1, G)
        def _(j):
            m = G - j
            e_copy(b, m).wait_recv()

            @pl.when(jnp.logical_and(m == far, b == z))
            def _():
                pl.when(z < L - 2)(f_copy(0).start)
                pl.when(z > 1)(f_copy(1).start)

            d_copy(b, m).start()

        @pl.loop(0, G)
        def _(m):
            d_copy(b, m).wait_recv()

        for i in range(2):
            w_load(s, i).wait()

        @pl.loop(0, rows // tile)
        def _(t):
            at = pl.ds(pl.multiple_of(t * tile, 16), tile)
            both = gate_up(b, slot, at)

            @pl.when(s == 0)
            def _():
                for i in range(2):
                    acc[i, at] = both[i]

            @pl.when(s > 0)
            def _():
                for i in range(2):
                    acc[i, at] += both[i]

        @pl.when(s + 2 < L)
        def _():
            for i in range(2):
                w_load(s + 2, i).start()

    process(0)

    @pl.loop(1, L)
    def _(s):
        @pl.when(jnp.logical_or(jnp.logical_not(inside), s == 1))
        def _():
            take(s)
            pl.when(inside)(lambda: take(s + 1))
            process(s)

        @pl.when(jnp.logical_and(inside, s + 1 < L))
        def _():
            pl.when(s > 1)(lambda: take(s + 1))
            process(s + 1)

        @pl.when(jnp.logical_and(next_to_end, s == L - 1))
        def _():
            e_copy(farthest, far).wait_recv()
            l_copy().start()

        finish(s - 1)

    def extra(b, side):
        if side == 0:
            return jnp.logical_and(z > 0, b == jnp.where(z > 1, z, L - 1))
        return jnp.logical_and(z < L - 1, b == jnp.where(z < L - 2, z, 0))

    def add_extra(b):
        for side in range(2):
            @pl.when(extra(b, side))
            def _():
                a_copy(b, side).wait_recv()
                tbuf[0:cap] += abuf[side].astype(F32)

        obuf[b, far - 1] = tbuf[0:cap].astype(BF16)

    def project(i, m):
        b = order(L - 1 - i)
        at = group_rows(flip(g, m, G))
        if units % LANES == 0:
            left = jnp.concatenate([hbuf[0, at], hbuf[1, at]], axis=1)
            result = jnp.dot(left, dbuf[b], preferred_element_type=F32)
        else:
            result = jnp.dot(hbuf[0, at], dbuf[b, 0:units], preferred_element_type=F32)
            result += jnp.dot(hbuf[1, at], dbuf[b, units:], preferred_element_type=F32)

        @pl.when(m == 0)
        def _():
            rbuf[b, at] = result.astype(BF16)

        @pl.when(jnp.logical_and(m > 0, m < far))
        def _():
            e_copy(b, m).wait_send()
            obuf[b, m - 1] = result.astype(BF16)

        @pl.when(m == far)
        def _():
            @pl.when(skipped(b))
            def _():
                obuf[b, far - 1] = result.astype(BF16)
                to_right = jnp.where(inside, b > z, z == 0)
                pl.when(to_right)(a_copy(b, 0).start)
                pl.when(jnp.logical_not(to_right))(a_copy(b, 1).start)

            @pl.when(jnp.logical_not(skipped(b)))
            def _():
                e_copy(b, far).wait_send()
                tbuf[0:cap] = result

                @pl.when(i > 0)
                def _():
                    add_extra(b)

    def each_send(i, act):
        b = order(L - 1 - i)

        @pl.loop(0, G - 1)
        def _(j):
            m = far - j

            @pl.when(jnp.logical_not(jnp.logical_and(m == far, skipped(b))))
            def _():
                act(b, m)

    def start_sends(i):
        each_send(i, lambda b, m: r_copy(b, m).start())

    def wait_sends(i):
        each_send(i, lambda b, m: r_copy(b, m).wait_send())

    def down_ready(b):
        down_own(b).wait()
        down_push(b).wait_recv()

    def project_all(i):
        down_ready(order(L - 1 - i))

        @pl.loop(0, G)
        def _(j):
            project(i, G - 1 - j)

    last = order(L - 1)

    @pl.loop(1, G)
    def _(m):
        @pl.when(jnp.logical_not(jnp.logical_and(m == far, next_to_end)))
        def _():
            e_copy(last, m).wait_recv()

        d_copy(last, m).start()

    for i in range(2):
        w_load(L - 1, i).wait()
    down_ready(last)

    @pl.loop(0, G + 1)
    def _(q):
        @pl.when(q < G)
        def _():
            m = lax.rem(q + 1, G)
            d_copy(last, m).wait_recv()
            first = flip(g, m, G) * cap

            @pl.loop(0, cap // tile)
            def _(t):
                at = pl.ds(pl.multiple_of(first + t * tile, 16), tile)
                both = gate_up(last, (L - 1) % 2, at)
                gates = acc[0, at] + both[0]
                half = 0.5 * gates
                hbuf[core, at] = ((half + half * jnp.tanh(half)) * (acc[1, at] + both[1])).astype(BF16)

            h_copy(m).start()

        @pl.when(q > 0)
        def _():
            m = lax.rem(q, G)
            h_copy(m).wait_recv()
            project(0, m)
            direct = jnp.logical_and(m > 0, m < far)
            pl.when(direct)(lambda: r_copy(last, m).start())

            @pl.when(jnp.logical_and(m == far, jnp.logical_not(jnp.logical_or(skipped(last), next_to_end))))
            def _():
                obuf[last, far - 1] = tbuf[0:cap].astype(BF16)
                r_copy(last, far).start()

    @pl.when(next_to_end)
    def _():
        add_extra(last)
        r_copy(last, far).start()

    project_all(1)
    wait_sends(0)
    start_sends(1)

    pl.when(z < L - 1)(z_copy(z, 0).wait_send)
    pl.when(z > 0)(z_copy(z, 1).wait_send)
    pl.when(z < L - 2)(f_copy(0).wait_send)
    pl.when(z > 1)(f_copy(1).wait_send)
    pl.when(next_to_end)(l_copy().wait_send)

    @pl.loop(0, L)
    def _(b):
        pl.when(jnp.logical_and(b < z, z < L - 1))(z_copy(b, 0).wait_send)
        pl.when(jnp.logical_and(b > z, z > 0))(z_copy(b, 1).wait_send)

        @pl.loop(0, G)
        def _(m):
            d_copy(b, m).wait_send()

        @pl.when(skipped(b))
        def _():
            rbuf[b, group_rows(flip(g, far, G))] = jnp.zeros((cap, cols), BF16)

    per = rows // tok
    blocks = rows // cols

    def mix_place(k):
        return k // (L * per), (k // per) % L, (k % per) * tok

    for k in range(blocks):
        c, b, first = mix_place(k)
        lane = lax.broadcasted_iota(jnp.int32, (LANES, cols), 1) + k * cols
        for r in range(nb):
            value = jnp.zeros((LANES, cols), F32)
            for e in range(k * cols // cap, ((k + 1) * cols - 1) // cap + 1):
                q = e * nb + r
                value = jnp.where(kcol[:, q : q + 1] == lane, wcol[:, q : q + 1], value)
            piece[c, b, first + r * LANES : first + (r + 1) * LANES] = value.astype(BF16)

    step = min(256, tok)

    def combined(b, t):
        parts = []
        for k in range(blocks):
            c, l, first = mix_place(k)
            parts.append(piece[c, l, pl.ds(pl.multiple_of(first + t * step, 16), step)])
        return jnp.dot(jnp.concatenate(parts, axis=1), rbuf[b], preferred_element_type=F32)

    def arrived(b):
        @pl.loop(1, G)
        def _(m):
            @pl.when(jnp.logical_not(jnp.logical_and(m == far, skipped(b))))
            def _():
                r_copy(b, m).wait_recv()

    @pl.loop(0, L - 1)
    def _(i):
        @pl.when(i > 0)
        def _():
            wait_sends(i)
            start_sends(i + 1)

        pl.when(i + 2 < L)(lambda: project_all(i + 2))
        b = order(L - 1 - i)
        more = jnp.where(b > z, z, L - 1 - z) > 0
        arrived(b)

        @pl.when(more)
        def _():
            remote(zbuf.at[b], rin.at[b], ys.at[b], yr.at[b], at_z(b)).wait_recv()

        @pl.loop(0, tok // step)
        def _(t):
            at = pl.ds(pl.multiple_of(t * step, 16), step)
            value = combined(b, t)

            @pl.when(more)
            def _():
                zbuf[b, at] = (value + rin[b, at].astype(F32)).astype(BF16)

            @pl.when(jnp.logical_not(more))
            def _():
                zbuf[b, at] = value.astype(BF16)

        pl.when(b > z)(y_copy(b, 0).start)
        pl.when(b < z)(y_copy(b, 1).start)

    arrived(z)

    @pl.loop(0, tok // step)
    def _(t):
        at = pl.ds(pl.multiple_of(t * step, 16), step)
        tbuf[at] = combined(z, t)

    for side, slot in ((0, z), (1, L)):
        @pl.when(z > 0 if side == 0 else z < L - 1)
        def _():
            remote(zbuf.at[z], rin.at[slot], ys.at[z], yr.at[slot], partner).wait_recv()
            tbuf[...] += rin[slot].astype(F32)

    stat2[me] = squares_of(tbuf[...], nb)
    for k in range(1, n):
        stat_copy(stat2, ts, tr, k).start()
    post = post_ref[...].astype(F32).reshape(1, cols)
    scol[...] = row_scale(stat2, ts, tr)
    for r in range(nb):
        at = slice(r * LANES, (r + 1) * LANES)
        nbuf[at] = (tbuf[at] * scol[:, r : r + 1] * post).astype(BF16)
    out_copy = pltpu.make_async_copy(nbuf, out_ref, xs.at[0])
    out_copy.start()

    for k in range(1, n):
        stat_copy(stat, ss, sr, k).wait_send()
        stat_copy(stat2, ts, tr, k).wait_send()

    pl.when(z == 0)(a_copy(farthest, 0).wait_send)
    pl.when(z == L - 1)(a_copy(farthest, 1).wait_send)

    @pl.when(inside)
    def _():
        a_copy(z + 1, 0).wait_send()
        a_copy(z - 1, 1).wait_send()

    wait_sends(L - 1)

    @pl.loop(0, L)
    def _(b):
        down_push(b).wait_send()
        pl.when(b > z)(y_copy(b, 0).wait_send)
        pl.when(b < z)(y_copy(b, 1).wait_send)

    @pl.loop(0, G)
    def _(m):
        h_copy(m).wait_send()

    out_copy.wait()


def on_device(
    tokens, pre_gain, route_ids, route_weights, gate_weight, up_weight, down_weight, post_gain
):
    tok, cols = tokens.shape
    top = route_ids.shape[1]
    G = lax.axis_size("ep")
    n = lax.axis_size("tp")
    L = n // 2
    cap = 9 * tok * top // (8 * G)
    rows = G * cap
    units = gate_weight.shape[2]
    nb = tok // LANES
    tile = cap
    vmem = pl.BlockSpec(memory_space=pltpu.VMEM)
    hbm = pl.BlockSpec(memory_space=pl.ANY)
    return pl.pallas_call(
        functools.partial(layer_kernel, L, G, cap, tile),
        out_shape=jax.ShapeDtypeStruct((tok, cols), BF16),
        in_specs=[hbm] + [vmem] * 4 + [hbm] * 3,
        out_specs=hbm,
        scratch_shapes=[
            pltpu.VMEM((L, tok, cols), BF16),
            pltpu.VMEM((tok, cols), BF16),
            pltpu.VMEM((L, G - 1, cap, cols), BF16),
            pltpu.VMEM((2, L, rows, cols), BF16),
            pltpu.VMEM((2, 2, 2 * cols, units), BF16),
            pltpu.VMEM((2, rows, units), F32),
            pltpu.VMEM((2, rows, units), BF16),
            pltpu.VMEM((L, 2 * units, cols), BF16),
            pltpu.VMEM((L, rows, cols), BF16),
            pltpu.VMEM((L + 1, tok, cols), BF16),
            pltpu.VMEM((2, cap, cols), BF16),
            pltpu.VMEM((tok, cols), F32),
            pltpu.VMEM((n, 2 * nb, LANES), F32),
            pltpu.VMEM((n, nb, LANES), F32),
            pltpu.VMEM((G * nb, LANES), jnp.int32),
            pltpu.VMEM((LANES, LANES), jnp.int32),
            pltpu.VMEM((LANES, LANES), F32),
            pltpu.VMEM((LANES, LANES), F32),
            DMA((2, L)), DMA((L,)),
            DMA((L, G)), DMA((L, G)),
            DMA((3,)),
            DMA((L, G)), DMA((L, G)),
            DMA((2, 2)),
            DMA((L,)), DMA((L,)), DMA((L,)),
            DMA((G,)), DMA((G,)),
            DMA((L, G)), DMA((L, G)),
            DMA((2,)), DMA((2,)),
            DMA((L,)), DMA((L + 1,)),
            DMA((n,)), DMA((n,)),
            DMA((n,)), DMA((n,)),
            DMA((1,)),
        ],
        compiler_params=pltpu.CompilerParams(
            collective_id=1, has_side_effects=True, vmem_limit_bytes=62 * 2**20
        ),
        name="layer",
    )(
        tokens, pre_gain, post_gain, route_ids.T, route_weights.T,
        gate_weight[0], up_weight[0], down_weight[0],
    )


def solution(mesh):
    placed = (
        P("ep", "tp"),
        P("tp"),
        P("ep", None),
        P("ep", None),
        P("ep", None, "tp"),
        P("ep", None, "tp"),
        P("ep", "tp", None),
        P("tp"),
    )
    return jax.shard_map(
        on_device, mesh=mesh, in_specs=placed, out_specs=P("ep", "tp"), check_vma=False
    )
```

```python
import functools

import jax
import jax.numpy as jnp
from jax import lax
from jax.experimental import pallas as pl
from jax.experimental.pallas import tpu as pltpu
from jax.sharding import PartitionSpec as P

epsilon = 1e-06
MESH = pl.DeviceIdType.MESH
DMA = pltpu.SemaphoreType.DMA
BF16 = jnp.bfloat16
F32 = jnp.float32
LANES = 128


def flip(a, m, size):
    total, bit = 0, 1
    while bit < size:
        total = total + (((a // bit) % 2 + (m // bit) % 2) % 2) * bit
        bit *= 2
    return total


def columns_of(values):
    rows = values.shape[0]
    if rows < LANES:
        values = jnp.concatenate([values, jnp.zeros((LANES - rows, LANES), values.dtype)], axis=0)
    return values.T


def fold(wide, nb):
    row = lax.broadcasted_iota(jnp.int32, (nb, LANES), 0)
    total = None
    for r in range(nb):
        part = jnp.broadcast_to(wide[:, r * LANES : (r + 1) * LANES], (nb, LANES))
        total = part if total is None else jnp.where(row == r, part, total)
    return total


def squares_of(v, nb):
    square = v * v
    high = square.astype(BF16)
    low = (square - high.astype(F32)).astype(BF16)
    ones = jnp.ones((nb, v.shape[1]), BF16)
    dims = (((1,), (1,)), ((), ()))
    wide = lax.dot_general(ones, high, dims, preferred_element_type=F32)
    wide += lax.dot_general(ones, low, dims, preferred_element_type=F32)
    return fold(wide, nb)


def layer_kernel(
    L, G, cap, tile,
    x_ref, pre_ref, post_ref, ids_ref, rw_ref, gate_ref, up_ref, down_ref, out_ref,
    zbuf, nbuf, obuf, piece, wbuf, acc, hbuf, dbuf, rbuf, rin, abuf, ebuf, tbuf,
    stat, stat2, kbuf, kcol, wcol, scol,
    zs, zr, es, er, fs, ds, dr, ws, dl, dps, dpr, hs, hr, rs, rr, as_, ar, ys, yr, ss, sr, ts, tr, xs,
):
    tok, cols = nbuf.shape
    nb = tok // LANES
    n = 2 * L
    units = gate_ref.shape[1]
    rows = G * cap
    far = G - 1
    me, g = lax.axis_index("tp"), lax.axis_index("ep")
    core, z = lax.rem(me, 2), me // 2
    partner = {"tp": me + 1 - 2 * core}
    inside = jnp.logical_and(z > 0, z < L - 1)
    inner = jnp.minimum(z, L - 1 - z)
    width = n * cols
    step = min(256, tok)
    tiles = tok // step

    def order(s):
        near = jnp.where(s % 2 == 1, z - (s + 1) // 2, z + (s + 1) // 2)
        rest = jnp.where(2 * z > L - 1, z - (s - inner), z + (s - inner))
        return jnp.where(s <= 2 * inner, near, rest)

    farthest = jnp.where(2 * z > L - 1, 0, L - 1)
    last = order(L - 1)
    end_left = z == 1
    next_to_end = jnp.logical_or(z == 1, z == L - 2)

    def skipped(b):
        beside = jnp.logical_or(b == z + 1, b == z - 1)
        return jnp.where(inside, beside, b == farthest)

    def group_rows(e):
        return pl.ds(pl.multiple_of(e * cap, 16), cap)

    def remote(src, dst, send, recv, to):
        return pltpu.make_async_remote_copy(
            src_ref=src, dst_ref=dst, send_sem=send, recv_sem=recv, device_id=to, device_id_type=MESH
        )

    def at_z(to):
        return {"tp": to * 2 + core}

    def at_g(m):
        return {"ep": flip(g, m, G)}

    def w_load(s, i):
        ref = (gate_ref, up_ref)[i]
        depth = pl.ds(pl.multiple_of(order(s) * 2 * cols, LANES), 2 * cols)
        return pltpu.make_async_copy(ref.at[depth], wbuf.at[s % 2, i], ws.at[s % 2, i])

    def my_units(c):
        return pl.ds(pl.multiple_of(c * units, 16), units)

    def down_part(b, c):
        return down_ref.at[:, pl.ds(pl.multiple_of((b * 2 + c) * cols, LANES), cols)]

    def down_own(b):
        return pltpu.make_async_copy(down_part(b, core), dbuf.at[b, my_units(core)], dl.at[b])

    def down_push(b):
        return remote(
            down_part(b, 1 - core), dbuf.at[b, my_units(core)], dps.at[b], dpr.at[b], partner
        )

    def z_copy(b, side):
        return remote(zbuf.at[b], zbuf.at[b], zs.at[side, b], zr.at[b], at_z(z + 1 - 2 * side))

    def e_copy(b, m):
        return remote(
            obuf.at[b, m - 1], piece.at[core, b, group_rows(g)], es.at[b, m], er.at[b, m], at_g(m)
        )

    def f_copy(side):
        area = piece.at[core, z, group_rows(flip(g, far, G))]
        return remote(area, area, fs.at[side], er.at[z, far], at_z(z + 1 - 2 * side))

    def l_copy():
        area = piece.at[core, farthest, group_rows(flip(g, far, G))]
        return remote(area, area, fs.at[2], er.at[farthest, far], at_z(jnp.where(end_left, 0, L - 1)))

    def d_copy(b, m):
        area = piece.at[core, b, group_rows(flip(g, m, G))]
        return remote(area, area, ds.at[b, m], dr.at[b, m], partner)

    def h_copy(m):
        area = hbuf.at[core, group_rows(flip(g, m, G))]
        return remote(area, area, hs.at[m], hr.at[m], partner)

    def r_copy(b, m):
        return remote(
            obuf.at[b, m - 1], rbuf.at[b, group_rows(g)], rs.at[b, m], rr.at[b, m], at_g(m)
        )

    def a_copy(b, side):
        return remote(obuf.at[b, far - 1], abuf.at[side], as_.at[side], ar.at[side], at_z(z + 1 - 2 * side))

    def rows_of(t):
        return pl.ds(pl.multiple_of(t * step, 16), step)

    def y_copy(b, side, t):
        to = z + 1 - 2 * side
        slot = jnp.where(jnp.logical_and(to == b, side == 1), L, b)
        return remote(zbuf.at[b, rows_of(t)], rin.at[slot, rows_of(t)], ys.at[b, t], yr.at[slot, t], at_z(to))

    def y_wait(slot, t):
        area = rin.at[slot, rows_of(t)]
        remote(area, area, ys.at[0, t], yr.at[slot, t], partner).wait_recv()

    def stat_copy(buf, send, recv, k):
        to = lax.rem(me + k, n)
        return remote(buf.at[me], buf.at[me], send.at[to], recv.at[me], {"tp": to})

    def stat_wait(buf, send, recv, k):
        of = lax.rem(me + n - k, n)
        remote(buf.at[of], buf.at[of], send.at[of], recv.at[of], {"tp": of}).wait_recv()

    barrier = pltpu.get_barrier_semaphore()
    for k in range(1, n):
        pl.semaphore_signal(barrier, inc=1, device_id={"tp": lax.rem(me + k, n)}, device_id_type=MESH)
    for m in range(1, G):
        pl.semaphore_signal(barrier, inc=1, device_id=at_g(m), device_id_type=MESH)
    x_load = pltpu.make_async_copy(x_ref, zbuf.at[z], xs.at[0])
    x_load.start()
    for s in range(2):
        for i in range(2):
            w_load(s, i).start()

    @pl.loop(0, L)
    def _(b):
        down_own(b).start()

    x_load.wait()
    stat[me, 0:nb] = squares_of(zbuf[z].astype(F32), nb)
    pre = pre_ref[...].astype(F32).reshape(1, cols)
    for c in range(cols // LANES):
        stat[me, nb + c : nb + c + 1] = pre[:, c * LANES : (c + 1) * LANES]

    pl.semaphore_wait(barrier, n + G - 2)
    for k in range(1, n):
        stat_copy(stat, ss, sr, k).start()
    pl.when(z < L - 1)(z_copy(z, 0).start)
    pl.when(z > 0)(z_copy(z, 1).start)

    ids, weights = ids_ref[...], rw_ref[...]
    top = ids.shape[0]
    id_rows = [fold(ids[t : t + 1], nb) for t in range(top)]
    weight_rows = [fold(weights[t : t + 1], nb) for t in range(top)]
    members, shares = [], []
    for e in range(G):
        named = [r == e for r in id_rows]
        members.append(sum(jnp.where(q, 1.0, 0.0) for q in named))
        shares.append(sum(jnp.where(q, w, 0.0) for q, w in zip(named, weight_rows)))
    member = jnp.concatenate(members, axis=0)
    small = member.astype(BF16)
    lane_a = lax.broadcasted_iota(jnp.int32, (LANES, LANES), 0)
    lane_b = lax.broadcasted_iota(jnp.int32, (LANES, LANES), 1)
    both = jnp.concatenate(
        [jnp.where(lane_a < lane_b, 1.0, 0.0).astype(BF16), jnp.ones((LANES, LANES), BF16)], axis=1
    )
    counted = jnp.dot(small, both, preferred_element_type=F32)
    row_a = lax.broadcasted_iota(jnp.int32, (G * nb, G * nb), 0)
    row_b = lax.broadcasted_iota(jnp.int32, (G * nb, G * nb), 1)
    ahead = jnp.where(jnp.logical_and(row_a // nb == row_b // nb, row_b < row_a), 1.0, 0.0).astype(BF16)
    rank = counted[:, :LANES] + jnp.dot(
        ahead, counted[:, LANES:].astype(BF16), preferred_element_type=F32
    )
    base = (lax.broadcasted_iota(jnp.int32, (G * nb, LANES), 0) // nb * cap).astype(F32)
    key = jnp.where(member > 0.5, rank + base, -1.0)
    kbuf[...] = key.astype(jnp.int32)
    kcol[...] = columns_of(key).astype(jnp.int32)
    wcol[...] = columns_of(jnp.concatenate(shares, axis=0))

    for e in range(G):
        wanted = lax.broadcasted_iota(jnp.int32, (cap, LANES), 0) + e * cap
        for r in range(nb):
            l, lane = r * LANES // cols, r * LANES % cols
            rbuf[l, e * cap : (e + 1) * cap, lane : lane + LANES] = jnp.where(
                kbuf[e * nb + r : e * nb + r + 1] == wanted, 1.0, 0.0
            ).astype(BF16)

    def row_scale(buf, send, recv):
        for k in range(1, n):
            stat_wait(buf, send, recv, k)
        total = buf[0, 0:nb]
        for k in range(1, n):
            total = total + buf[k, 0:nb]
        return columns_of(lax.rsqrt(total / width + epsilon))

    scol[...] = row_scale(stat, ss, sr)

    @pl.loop(0, L)
    def _(b):
        down_push(b).start()

    def take(s):
        b = order(s)
        z_copy(b, 0).wait_recv()
        pl.when(jnp.logical_and(b < z, z < L - 1))(z_copy(b, 0).start)
        pl.when(jnp.logical_and(b > z, z > 0))(z_copy(b, 1).start)

    def process(s):
        b = order(s)
        gain = jnp.concatenate(
            [stat[b * 2 + core, nb + c : nb + c + 1] for c in range(cols // LANES)], axis=1
        )
        for r in range(nb):
            at = slice(r * LANES, (r + 1) * LANES)
            nbuf[at] = (zbuf[b, at].astype(F32) * scol[:, r : r + 1] * gain).astype(BF16)

        @pl.loop(0, G)
        def _(j):
            m = G - 1 - j

            @pl.when(jnp.logical_not(jnp.logical_and(m == far, skipped(b))))
            def _():
                at = group_rows(flip(g, m, G))
                chooser = jnp.concatenate([rbuf[l, at] for l in range(tok // cols)], axis=1)
                chosen = jnp.dot(chooser, nbuf[...], preferred_element_type=F32).astype(BF16)

                @pl.when(m > 0)
                def _():
                    obuf[b, m - 1] = chosen
                    e_copy(b, m).start()

                @pl.when(m == 0)
                def _():
                    piece[core, b, group_rows(g)] = chosen
                    d_copy(b, 0).start()

    def gate_up(b, slot, at):
        left = jnp.concatenate([piece[0, b, at], piece[1, b, at]], axis=1)
        return [jnp.dot(left, wbuf[slot, i], preferred_element_type=F32) for i in range(2)]

    per = rows // tok
    blocks = rows // cols

    def mix_place(k):
        return k // per % 2, order(k // (2 * per)), (k % per) * tok

    def build_mix(q):
        b = order(q)

        @pl.loop(0, G)
        def _(m):
            d_copy(b, m).wait_send()

        if q == 0:
            pl.when(z < L - 2)(f_copy(0).wait_send)
            pl.when(z > 1)(f_copy(1).wait_send)
        for k in range(2 * per * q, min(2 * per * (q + 1), blocks)):
            c, b, first = mix_place(k)
            lane = lax.broadcasted_iota(jnp.int32, (LANES, cols), 1) + k * cols
            for r in range(nb):
                value = jnp.zeros((LANES, cols), F32)
                for e in range(k * cols // cap, ((k + 1) * cols - 1) // cap + 1):
                    p = e * nb + r
                    value = jnp.where(kcol[:, p : p + 1] == lane, wcol[:, p : p + 1], value)
                piece[c, b, first + r * LANES : first + (r + 1) * LANES] = value.astype(BF16)

    def ready_last():
        @pl.loop(1, G)
        def _(m):
            @pl.when(jnp.logical_not(jnp.logical_and(m == far, next_to_end)))
            def _():
                e_copy(last, m).wait_recv()

            d_copy(last, m).start()

    def finish(s):
        b, slot = order(s), s % 2

        for q in range(L - 2):
            pl.when(s == q + 1)(functools.partial(build_mix, q))

        @pl.loop(1, G)
        def _(j):
            m = G - j
            e_copy(b, m).wait_recv()

            @pl.when(jnp.logical_and(m == far, b == z))
            def _():
                pl.when(z < L - 2)(f_copy(0).start)
                pl.when(z > 1)(f_copy(1).start)

            d_copy(b, m).start()

        @pl.loop(0, G)
        def _(m):
            d_copy(b, m).wait_recv()

        for i in range(2):
            w_load(s, i).wait()

        @pl.loop(0, rows // tile)
        def _(t):
            at = pl.ds(pl.multiple_of(t * tile, 16), tile)
            pl.when(jnp.logical_and(s == L - 2, t == rows // tile // 2))(ready_last)
            both = gate_up(b, slot, at)

            @pl.when(s == 0)
            def _():
                for i in range(2):
                    acc[i, at] = both[i]

            @pl.when(s > 0)
            def _():
                for i in range(2):
                    acc[i, at] += both[i]

        @pl.when(s + 2 < L)
        def _():
            for i in range(2):
                w_load(s + 2, i).start()

    process(0)

    @pl.loop(1, L)
    def _(s):
        @pl.when(jnp.logical_or(jnp.logical_not(inside), s == 1))
        def _():
            take(s)
            pl.when(inside)(lambda: take(s + 1))
            process(s)

        @pl.when(jnp.logical_and(inside, s + 1 < L))
        def _():
            pl.when(s > 1)(lambda: take(s + 1))
            process(s + 1)

        @pl.when(jnp.logical_and(next_to_end, s == L - 1))
        def _():
            e_copy(farthest, far).wait_recv()
            l_copy().start()

        finish(s - 1)

    def extra(b, side):
        if side == 0:
            return jnp.logical_and(z > 0, b == jnp.where(z > 1, z, L - 1))
        return jnp.logical_and(z < L - 1, b == jnp.where(z < L - 2, z, 0))

    def add_extra(b, held):
        for side in range(2):
            @pl.when(extra(b, side))
            def _():
                a_copy(b, side).wait_recv()
                held[0:cap] += abuf[side].astype(F32)

        obuf[b, far - 1] = held[0:cap].astype(BF16)

    def project(i, m):
        b = order(L - 1 - i)
        at = group_rows(flip(g, m, G))
        if units % LANES == 0:
            left = jnp.concatenate([hbuf[0, at], hbuf[1, at]], axis=1)
            result = jnp.dot(left, dbuf[b], preferred_element_type=F32)
        else:
            result = jnp.dot(hbuf[0, at], dbuf[b, 0:units], preferred_element_type=F32)
            result += jnp.dot(hbuf[1, at], dbuf[b, units:], preferred_element_type=F32)

        @pl.when(m == 0)
        def _():
            rbuf[b, at] = result.astype(BF16)

        @pl.when(jnp.logical_and(m > 0, m < far))
        def _():
            e_copy(b, m).wait_send()
            obuf[b, m - 1] = result.astype(BF16)

        @pl.when(m == far)
        def _():
            @pl.when(skipped(b))
            def _():
                obuf[b, far - 1] = result.astype(BF16)
                to_right = jnp.where(inside, b > z, z == 0)
                pl.when(to_right)(a_copy(b, 0).start)
                pl.when(jnp.logical_not(to_right))(a_copy(b, 1).start)

            @pl.when(jnp.logical_not(skipped(b)))
            def _():
                e_copy(b, far).wait_send()

                @pl.when(i > 0)
                def _():
                    tbuf[0:cap] = result

                @pl.when(i == 0)
                def _():
                    ebuf[...] = result

    def each_send(i, act):
        b = order(L - 1 - i)

        @pl.loop(0, G - 1)
        def _(j):
            m = far - j

            @pl.when(jnp.logical_not(jnp.logical_and(m == far, skipped(b))))
            def _():
                act(b, m)

    def start_sends(i):
        each_send(i, lambda b, m: r_copy(b, m).start())

    def wait_sends(i):
        each_send(i, lambda b, m: r_copy(b, m).wait_send())

    def down_ready(b):
        down_own(b).wait()
        down_push(b).wait_recv()

    def project_all(i):
        down_ready(order(L - 1 - i))

        @pl.loop(0, G)
        def _(j):
            project(i, G - 1 - j)

    build_mix(L - 2)
    for i in range(2):
        w_load(L - 1, i).wait()
    down_ready(last)

    @pl.loop(0, G + 1)
    def _(q):
        @pl.when(q < G)
        def _():
            m = lax.rem(q + 1, G)
            d_copy(last, m).wait_recv()
            first = flip(g, m, G) * cap

            @pl.loop(0, cap // tile)
            def _(t):
                at = pl.ds(pl.multiple_of(first + t * tile, 16), tile)
                both = gate_up(last, (L - 1) % 2, at)
                gates = acc[0, at] + both[0]
                half = 0.5 * gates
                hbuf[core, at] = ((half + half * jnp.tanh(half)) * (acc[1, at] + both[1])).astype(BF16)

            h_copy(m).start()

        @pl.when(q > 0)
        def _():
            m = lax.rem(q, G)
            h_copy(m).wait_recv()
            project(0, m)
            direct = jnp.logical_and(m > 0, m < far)
            pl.when(direct)(lambda: r_copy(last, m).start())

            @pl.when(jnp.logical_and(m == far, jnp.logical_not(jnp.logical_or(skipped(last), next_to_end))))
            def _():
                obuf[last, far - 1] = ebuf[...].astype(BF16)
                r_copy(last, far).start()

    pl.when(z < L - 1)(z_copy(z, 0).wait_send)
    pl.when(z > 0)(z_copy(z, 1).wait_send)
    pl.when(next_to_end)(l_copy().wait_send)

    @pl.loop(0, L)
    def _(b):
        pl.when(jnp.logical_and(b < z, z < L - 1))(z_copy(b, 0).wait_send)
        pl.when(jnp.logical_and(b > z, z > 0))(z_copy(b, 1).wait_send)

        @pl.when(skipped(b))
        def _():
            rbuf[b, group_rows(flip(g, far, G))] = jnp.zeros((cap, cols), BF16)

    def combined(b, t):
        parts = []
        for k in range(blocks):
            c, l, first = mix_place(k)
            parts.append(piece[c, l, pl.ds(pl.multiple_of(first + t * step, 16), step)])
        return jnp.dot(jnp.concatenate(parts, axis=1), rbuf[b], preferred_element_type=F32)

    def arrived(b):
        @pl.loop(1, G)
        def _(m):
            @pl.when(jnp.logical_not(jnp.logical_and(m == far, skipped(b))))
            def _():
                r_copy(b, m).wait_recv()

    def combine(i):
        b = order(L - 1 - i)
        more = jnp.where(b > z, z, L - 1 - z) > 0
        arrived(b)

        @pl.loop(0, tiles)
        def _(t):
            at = rows_of(t)
            value = combined(b, t)

            @pl.when(more)
            def _():
                y_wait(b, t)
                zbuf[b, at] = (value + rin[b, at].astype(F32)).astype(BF16)

            @pl.when(jnp.logical_not(more))
            def _():
                zbuf[b, at] = value.astype(BF16)

            pl.when(b > z)(y_copy(b, 0, t).start)
            pl.when(b < z)(y_copy(b, 1, t).start)

    @pl.loop(1, L)
    def _(i):
        b = order(L - 1 - i)
        project_all(i)
        pl.when(jnp.logical_or(i > 1, jnp.logical_not(inside)))(lambda: wait_sends(i - 1))
        pl.when(jnp.logical_not(skipped(b)))(lambda: add_extra(b, tbuf))
        start_sends(i)

        @pl.when(jnp.logical_and(next_to_end, i == 1))
        def _():
            add_extra(last, ebuf)
            r_copy(last, far).start()

        late = jnp.where(inside, 2, 1)
        pl.when(i >= late)(lambda: combine(i - late))

    pl.when(inside)(lambda: combine(L - 2))
    arrived(z)

    @pl.loop(0, tiles)
    def _(t):
        tbuf[rows_of(t)] = combined(z, t)

    @pl.loop(0, tiles)
    def _(t):
        at = rows_of(t)
        for side, slot in ((0, z), (1, L)):
            @pl.when(z > 0 if side == 0 else z < L - 1)
            def _():
                y_wait(slot, t)
                tbuf[at] += rin[slot, at].astype(F32)

    stat2[me] = squares_of(tbuf[...], nb)
    for k in range(1, n):
        stat_copy(stat2, ts, tr, k).start()
    post = post_ref[...].astype(F32).reshape(1, cols)
    scol[...] = row_scale(stat2, ts, tr)
    for r in range(nb):
        at = slice(r * LANES, (r + 1) * LANES)
        nbuf[at] = (tbuf[at] * scol[:, r : r + 1] * post).astype(BF16)
    out_copy = pltpu.make_async_copy(nbuf, out_ref, xs.at[0])
    out_copy.start()

    for k in range(1, n):
        stat_copy(stat, ss, sr, k).wait_send()
        stat_copy(stat2, ts, tr, k).wait_send()

    pl.when(z == 0)(a_copy(farthest, 0).wait_send)
    pl.when(z == L - 1)(a_copy(farthest, 1).wait_send)

    @pl.when(inside)
    def _():
        a_copy(z + 1, 0).wait_send()
        a_copy(z - 1, 1).wait_send()

    pl.when(inside)(lambda: wait_sends(0))
    wait_sends(L - 1)

    @pl.loop(0, L)
    def _(b):
        down_push(b).wait_send()

        @pl.loop(0, tiles)
        def _(t):
            pl.when(b > z)(y_copy(b, 0, t).wait_send)
            pl.when(b < z)(y_copy(b, 1, t).wait_send)

    @pl.loop(0, G)
    def _(m):
        d_copy(last, m).wait_send()

    @pl.loop(0, G)
    def _(m):
        h_copy(m).wait_send()

    out_copy.wait()


def on_device(
    tokens, pre_gain, route_ids, route_weights, gate_weight, up_weight, down_weight, post_gain
):
    tok, cols = tokens.shape
    top = route_ids.shape[1]
    G = lax.axis_size("ep")
    n = lax.axis_size("tp")
    L = n // 2
    cap = 9 * tok * top // (8 * G)
    rows = G * cap
    units = gate_weight.shape[2]
    nb = tok // LANES
    tile = cap
    tiles = tok // min(256, tok)
    vmem = pl.BlockSpec(memory_space=pltpu.VMEM)
    hbm = pl.BlockSpec(memory_space=pl.ANY)
    return pl.pallas_call(
        functools.partial(layer_kernel, L, G, cap, tile),
        out_shape=jax.ShapeDtypeStruct((tok, cols), BF16),
        in_specs=[hbm] + [vmem] * 4 + [hbm] * 3,
        out_specs=hbm,
        scratch_shapes=[
            pltpu.VMEM((L, tok, cols), BF16),
            pltpu.VMEM((tok, cols), BF16),
            pltpu.VMEM((L, G - 1, cap, cols), BF16),
            pltpu.VMEM((2, L, rows, cols), BF16),
            pltpu.VMEM((2, 2, 2 * cols, units), BF16),
            pltpu.VMEM((2, rows, units), F32),
            pltpu.VMEM((2, rows, units), BF16),
            pltpu.VMEM((L, 2 * units, cols), BF16),
            pltpu.VMEM((L, rows, cols), BF16),
            pltpu.VMEM((L + 1, tok, cols), BF16),
            pltpu.VMEM((2, cap, cols), BF16),
            pltpu.VMEM((cap, cols), F32),
            pltpu.VMEM((tok, cols), F32),
            pltpu.VMEM((n, 2 * nb, LANES), F32),
            pltpu.VMEM((n, nb, LANES), F32),
            pltpu.VMEM((G * nb, LANES), jnp.int32),
            pltpu.VMEM((LANES, LANES), jnp.int32),
            pltpu.VMEM((LANES, LANES), F32),
            pltpu.VMEM((LANES, LANES), F32),
            DMA((2, L)), DMA((L,)),
            DMA((L, G)), DMA((L, G)),
            DMA((3,)),
            DMA((L, G)), DMA((L, G)),
            DMA((2, 2)),
            DMA((L,)), DMA((L,)), DMA((L,)),
            DMA((G,)), DMA((G,)),
            DMA((L, G)), DMA((L, G)),
            DMA((2,)), DMA((2,)),
            DMA((L, tiles)), DMA((L + 1, tiles)),
            DMA((n,)), DMA((n,)),
            DMA((n,)), DMA((n,)),
            DMA((1,)),
        ],
        compiler_params=pltpu.CompilerParams(
            collective_id=1, has_side_effects=True, vmem_limit_bytes=62 * 2**20
        ),
        name="layer",
    )(
        tokens, pre_gain, post_gain, route_ids.T, route_weights.T,
        gate_weight[0], up_weight[0], down_weight[0],
    )


def solution(mesh):
    placed = (
        P("ep", "tp"),
        P("tp"),
        P("ep", None),
        P("ep", None),
        P("ep", None, "tp"),
        P("ep", None, "tp"),
        P("ep", "tp", None),
        P("tp"),
    )
    return jax.shard_map(
        on_device, mesh=mesh, in_specs=placed, out_specs=P("ep", "tp"), check_vma=False
    )
```

```python
import functools

import jax
import jax.numpy as jnp
from jax import lax
from jax.experimental import pallas as pl
from jax.experimental.pallas import tpu as pltpu
from jax.sharding import PartitionSpec as P

epsilon = 1e-06
MESH = pl.DeviceIdType.MESH
DMA = pltpu.SemaphoreType.DMA
BF16 = jnp.bfloat16
F32 = jnp.float32
LANES = 128


def flip(a, m, size):
    total, bit = 0, 1
    while bit < size:
        total = total + (((a // bit) % 2 + (m // bit) % 2) % 2) * bit
        bit *= 2
    return total


def columns_of(values):
    rows = values.shape[0]
    if rows < LANES:
        values = jnp.concatenate([values, jnp.zeros((LANES - rows, LANES), values.dtype)], axis=0)
    return values.T


def fold(wide, nb):
    row = lax.broadcasted_iota(jnp.int32, (nb, LANES), 0)
    total = None
    for r in range(nb):
        part = jnp.broadcast_to(wide[:, r * LANES : (r + 1) * LANES], (nb, LANES))
        total = part if total is None else jnp.where(row == r, part, total)
    return total


def squares_of(v, nb):
    square = v * v
    high = square.astype(BF16)
    low = (square - high.astype(F32)).astype(BF16)
    ones = jnp.ones((nb, v.shape[1]), BF16)
    dims = (((1,), (1,)), ((), ()))
    wide = lax.dot_general(ones, high, dims, preferred_element_type=F32)
    wide += lax.dot_general(ones, low, dims, preferred_element_type=F32)
    return fold(wide, nb)


def layer_kernel(
    L, G, cap, tile,
    x_ref, pre_ref, post_ref, ids_ref, rw_ref, gate_ref, up_ref, down_ref, out_ref,
    zbuf, nbuf, obuf, piece, wbuf, acc, hbuf, dbuf, rbuf, rin, abuf, ebuf, tbuf,
    stat, stat2, kbuf, kcol, wcol, scol,
    zs, zr, es, er, fs, ds, dr, ws, dl, dps, dpr, hs, hr, rs, rr, as_, ar, ys, yr, ss, sr, ts, tr, xs,
):
    tok, cols = nbuf.shape
    nb = tok // LANES
    n = 2 * L
    units = gate_ref.shape[1]
    rows = G * cap
    far = G - 1
    me, g = lax.axis_index("tp"), lax.axis_index("ep")
    core, z = lax.rem(me, 2), me // 2
    partner = {"tp": me + 1 - 2 * core}
    inside = jnp.logical_and(z > 0, z < L - 1)
    inner = jnp.minimum(z, L - 1 - z)
    width = n * cols
    step = min(256, tok)
    tiles = tok // step

    def order(s):
        near = jnp.where(s % 2 == 1, z - (s + 1) // 2, z + (s + 1) // 2)
        rest = jnp.where(2 * z > L - 1, z - (s - inner), z + (s - inner))
        return jnp.where(s <= 2 * inner, near, rest)

    farthest = jnp.where(2 * z > L - 1, 0, L - 1)
    last = order(L - 1)
    end_left = z == 1
    next_to_end = jnp.logical_or(z == 1, z == L - 2)

    def skipped(b):
        beside = jnp.logical_or(b == z + 1, b == z - 1)
        return jnp.where(inside, beside, b == farthest)

    def group_rows(e):
        return pl.ds(pl.multiple_of(e * cap, 16), cap)

    def remote(src, dst, send, recv, to):
        return pltpu.make_async_remote_copy(
            src_ref=src, dst_ref=dst, send_sem=send, recv_sem=recv, device_id=to, device_id_type=MESH
        )

    def at_z(to):
        return {"tp": to * 2 + core}

    def at_g(m):
        return {"ep": flip(g, m, G)}

    def w_load(s, i):
        ref = (gate_ref, up_ref)[i]
        depth = pl.ds(pl.multiple_of(order(s) * 2 * cols, LANES), 2 * cols)
        return pltpu.make_async_copy(ref.at[depth], wbuf.at[s % 2, i], ws.at[s % 2, i])

    def my_units(c):
        return pl.ds(pl.multiple_of(c * units, 16), units)

    def down_part(b, c):
        return down_ref.at[:, pl.ds(pl.multiple_of((b * 2 + c) * cols, LANES), cols)]

    def down_own(b):
        return pltpu.make_async_copy(down_part(b, core), dbuf.at[b, my_units(core)], dl.at[b])

    def down_push(b):
        return remote(
            down_part(b, 1 - core), dbuf.at[b, my_units(core)], dps.at[b], dpr.at[b], partner
        )

    def z_copy(b, side):
        return remote(zbuf.at[b], zbuf.at[b], zs.at[side, b], zr.at[b], at_z(z + 1 - 2 * side))

    def e_copy(b, m):
        return remote(
            obuf.at[b, m - 1], piece.at[core, b, group_rows(g)], es.at[b, m], er.at[b, m], at_g(m)
        )

    def f_copy(side):
        area = piece.at[core, z, group_rows(flip(g, far, G))]
        return remote(area, area, fs.at[side], er.at[z, far], at_z(z + 1 - 2 * side))

    def l_copy():
        area = piece.at[core, farthest, group_rows(flip(g, far, G))]
        return remote(area, area, fs.at[2], er.at[farthest, far], at_z(jnp.where(end_left, 0, L - 1)))

    def d_copy(b, m):
        area = piece.at[core, b, group_rows(flip(g, m, G))]
        return remote(area, area, ds.at[b, m], dr.at[b, m], partner)

    def h_copy(m):
        area = hbuf.at[core, group_rows(flip(g, m, G))]
        return remote(area, area, hs.at[m], hr.at[m], partner)

    def r_copy(b, m):
        return remote(
            obuf.at[b, m - 1], rbuf.at[b, group_rows(g)], rs.at[b, m], rr.at[b, m], at_g(m)
        )

    def a_copy(b, side):
        return remote(obuf.at[b, far - 1], abuf.at[side], as_.at[side], ar.at[side], at_z(z + 1 - 2 * side))

    def rows_of(t):
        return pl.ds(pl.multiple_of(t * step, 16), step)

    def y_copy(b, side, t):
        to = z + 1 - 2 * side
        slot = jnp.where(jnp.logical_and(to == b, side == 1), L, b)
        return remote(zbuf.at[b, rows_of(t)], rin.at[slot, rows_of(t)], ys.at[b, t], yr.at[slot, t], at_z(to))

    def y_wait(slot, t):
        area = rin.at[slot, rows_of(t)]
        remote(area, area, ys.at[0, t], yr.at[slot, t], partner).wait_recv()

    def stat_copy(buf, send, recv, k):
        to = lax.rem(me + k, n)
        return remote(buf.at[me], buf.at[me], send.at[to], recv.at[me], {"tp": to})

    def stat_wait(buf, send, recv, k):
        of = lax.rem(me + n - k, n)
        remote(buf.at[of], buf.at[of], send.at[of], recv.at[of], {"tp": of}).wait_recv()

    barrier = pltpu.get_barrier_semaphore()
    for k in range(1, n):
        pl.semaphore_signal(barrier, inc=1, device_id={"tp": lax.rem(me + k, n)}, device_id_type=MESH)
    for m in range(1, G):
        pl.semaphore_signal(barrier, inc=1, device_id=at_g(m), device_id_type=MESH)
    x_load = pltpu.make_async_copy(x_ref, zbuf.at[z], xs.at[0])
    x_load.start()
    for s in range(2):
        for i in range(2):
            w_load(s, i).start()

    @pl.loop(0, L)
    def _(b):
        down_own(b).start()

    x_load.wait()
    stat[me, 0:nb] = squares_of(zbuf[z].astype(F32), nb)
    pre = pre_ref[...].astype(F32).reshape(1, cols)
    for c in range(cols // LANES):
        stat[me, nb + c : nb + c + 1] = pre[:, c * LANES : (c + 1) * LANES]

    pl.semaphore_wait(barrier, n + G - 2)
    for k in range(1, n):
        stat_copy(stat, ss, sr, k).start()
    pl.when(z < L - 1)(z_copy(z, 0).start)
    pl.when(z > 0)(z_copy(z, 1).start)

    ids, weights = ids_ref[...], rw_ref[...]
    top = ids.shape[0]
    id_rows = [fold(ids[t : t + 1], nb) for t in range(top)]
    weight_rows = [fold(weights[t : t + 1], nb) for t in range(top)]
    members, shares = [], []
    for e in range(G):
        named = [r == e for r in id_rows]
        members.append(sum(jnp.where(q, 1.0, 0.0) for q in named))
        shares.append(sum(jnp.where(q, w, 0.0) for q, w in zip(named, weight_rows)))
    member = jnp.concatenate(members, axis=0)
    small = member.astype(BF16)
    lane_a = lax.broadcasted_iota(jnp.int32, (LANES, LANES), 0)
    lane_b = lax.broadcasted_iota(jnp.int32, (LANES, LANES), 1)
    both = jnp.concatenate(
        [jnp.where(lane_a < lane_b, 1.0, 0.0).astype(BF16), jnp.ones((LANES, LANES), BF16)], axis=1
    )
    counted = jnp.dot(small, both, preferred_element_type=F32)
    row_a = lax.broadcasted_iota(jnp.int32, (G * nb, G * nb), 0)
    row_b = lax.broadcasted_iota(jnp.int32, (G * nb, G * nb), 1)
    ahead = jnp.where(jnp.logical_and(row_a // nb == row_b // nb, row_b < row_a), 1.0, 0.0).astype(BF16)
    rank = counted[:, :LANES] + jnp.dot(
        ahead, counted[:, LANES:].astype(BF16), preferred_element_type=F32
    )
    base = (lax.broadcasted_iota(jnp.int32, (G * nb, LANES), 0) // nb * cap).astype(F32)
    key = jnp.where(member > 0.5, rank + base, -1.0)
    kbuf[...] = key.astype(jnp.int32)
    kcol[...] = columns_of(key).astype(jnp.int32)
    wcol[...] = columns_of(jnp.concatenate(shares, axis=0))

    for e in range(G):
        wanted = lax.broadcasted_iota(jnp.int32, (cap, LANES), 0) + e * cap
        for r in range(nb):
            l, lane = r * LANES // cols, r * LANES % cols
            rbuf[l, e * cap : (e + 1) * cap, lane : lane + LANES] = jnp.where(
                kbuf[e * nb + r : e * nb + r + 1] == wanted, 1.0, 0.0
            ).astype(BF16)

    def row_scale(buf, send, recv):
        for k in range(1, n):
            stat_wait(buf, send, recv, k)
        total = buf[0, 0:nb]
        for k in range(1, n):
            total = total + buf[k, 0:nb]
        return columns_of(lax.rsqrt(total / width + epsilon))

    scol[...] = row_scale(stat, ss, sr)

    @pl.loop(0, L)
    def _(b):
        down_push(b).start()

    def take(s):
        b = order(s)
        z_copy(b, 0).wait_recv()
        pl.when(jnp.logical_and(b < z, z < L - 1))(z_copy(b, 0).start)
        pl.when(jnp.logical_and(b > z, z > 0))(z_copy(b, 1).start)

    def process(s):
        b = order(s)
        gain = jnp.concatenate(
            [stat[b * 2 + core, nb + c : nb + c + 1] for c in range(cols // LANES)], axis=1
        )
        for r in range(nb):
            at = slice(r * LANES, (r + 1) * LANES)
            nbuf[at] = (zbuf[b, at].astype(F32) * scol[:, r : r + 1] * gain).astype(BF16)

        @pl.loop(0, G)
        def _(j):
            m = G - 1 - j

            @pl.when(jnp.logical_not(jnp.logical_and(m == far, skipped(b))))
            def _():
                at = group_rows(flip(g, m, G))
                chooser = jnp.concatenate([rbuf[l, at] for l in range(tok // cols)], axis=1)
                chosen = jnp.dot(chooser, nbuf[...], preferred_element_type=F32).astype(BF16)

                @pl.when(m > 0)
                def _():
                    obuf[b, m - 1] = chosen
                    e_copy(b, m).start()

                @pl.when(m == 0)
                def _():
                    piece[core, b, group_rows(g)] = chosen
                    d_copy(b, 0).start()

    def gate_up(b, slot, at):
        left = jnp.concatenate([piece[0, b, at], piece[1, b, at]], axis=1)
        return [jnp.dot(left, wbuf[slot, i], preferred_element_type=F32) for i in range(2)]

    per = rows // tok
    blocks = rows // cols

    def mix_place(k):
        return k // per % 2, order(k // (2 * per)), (k % per) * tok

    def build_mix(q):
        b = order(q)

        @pl.loop(0, G)
        def _(m):
            d_copy(b, m).wait_send()

        if q == 0:
            pl.when(z < L - 2)(f_copy(0).wait_send)
            pl.when(z > 1)(f_copy(1).wait_send)
        for k in range(2 * per * q, min(2 * per * (q + 1), blocks)):
            c, b, first = mix_place(k)
            lane = lax.broadcasted_iota(jnp.int32, (LANES, cols), 1) + k * cols
            for r in range(nb):
                value = jnp.zeros((LANES, cols), F32)
                for e in range(k * cols // cap, ((k + 1) * cols - 1) // cap + 1):
                    p = e * nb + r
                    value = jnp.where(kcol[:, p : p + 1] == lane, wcol[:, p : p + 1], value)
                piece[c, b, first + r * LANES : first + (r + 1) * LANES] = value.astype(BF16)

    def finish(s):
        b, slot = order(s), s % 2

        for q in range(L - 3):
            pl.when(s == q + 1)(functools.partial(build_mix, q))

        @pl.loop(1, G)
        def _(j):
            m = G - j
            e_copy(b, m).wait_recv()

            @pl.when(jnp.logical_and(m == far, b == z))
            def _():
                pl.when(z < L - 2)(f_copy(0).start)
                pl.when(z > 1)(f_copy(1).start)

            d_copy(b, m).start()

        @pl.loop(0, G)
        def _(m):
            d_copy(b, m).wait_recv()

        for i in range(2):
            w_load(s, i).wait()

        @pl.loop(0, rows // tile)
        def _(t):
            at = pl.ds(pl.multiple_of(t * tile, 16), tile)
            both = gate_up(b, slot, at)

            @pl.when(s == 0)
            def _():
                for i in range(2):
                    acc[i, at] = both[i]

            @pl.when(s > 0)
            def _():
                for i in range(2):
                    acc[i, at] += both[i]

        @pl.when(s + 2 < L)
        def _():
            for i in range(2):
                w_load(s + 2, i).start()

    process(0)

    @pl.loop(1, L)
    def _(s):
        @pl.when(jnp.logical_or(jnp.logical_not(inside), s == 1))
        def _():
            take(s)
            pl.when(inside)(lambda: take(s + 1))
            process(s)

        @pl.when(jnp.logical_and(inside, s + 1 < L))
        def _():
            pl.when(s > 1)(lambda: take(s + 1))
            process(s + 1)

        @pl.when(jnp.logical_and(next_to_end, s == L - 1))
        def _():
            e_copy(farthest, far).wait_recv()
            l_copy().start()

        pl.when(s < L - 1)(lambda: finish(s - 1))

    def extra(b, side):
        if side == 0:
            return jnp.logical_and(z > 0, b == jnp.where(z > 1, z, L - 1))
        return jnp.logical_and(z < L - 1, b == jnp.where(z < L - 2, z, 0))

    def add_extra(b, held):
        for side in range(2):
            @pl.when(extra(b, side))
            def _():
                a_copy(b, side).wait_recv()
                held[0:cap] += abuf[side].astype(F32)

        obuf[b, far - 1] = held[0:cap].astype(BF16)

    def project(i, m):
        b = order(L - 1 - i)
        at = group_rows(flip(g, m, G))
        if units % LANES == 0:
            left = jnp.concatenate([hbuf[0, at], hbuf[1, at]], axis=1)
            result = jnp.dot(left, dbuf[b], preferred_element_type=F32)
        else:
            result = jnp.dot(hbuf[0, at], dbuf[b, 0:units], preferred_element_type=F32)
            result += jnp.dot(hbuf[1, at], dbuf[b, units:], preferred_element_type=F32)

        @pl.when(m == 0)
        def _():
            rbuf[b, at] = result.astype(BF16)

        @pl.when(jnp.logical_and(m > 0, m < far))
        def _():
            e_copy(b, m).wait_send()
            obuf[b, m - 1] = result.astype(BF16)

        @pl.when(m == far)
        def _():
            @pl.when(skipped(b))
            def _():
                obuf[b, far - 1] = result.astype(BF16)
                to_right = jnp.where(inside, b > z, z == 0)
                pl.when(to_right)(a_copy(b, 0).start)
                pl.when(jnp.logical_not(to_right))(a_copy(b, 1).start)

            @pl.when(jnp.logical_not(skipped(b)))
            def _():
                e_copy(b, far).wait_send()

                @pl.when(i > 0)
                def _():
                    tbuf[0:cap] = result

                @pl.when(i == 0)
                def _():
                    ebuf[...] = result

    def sent(b, m):
        return jnp.logical_not(jnp.logical_and(m == far, skipped(b)))

    def wait_sends(i):
        b = order(L - 1 - i)

        @pl.loop(1, G)
        def _(m):
            pl.when(sent(b, m))(lambda: r_copy(b, m).wait_send())

    def start_sends(i):
        b = order(L - 1 - i)

        @pl.loop(0, far)
        def _(j):
            m = far - j
            pl.when(sent(b, m))(lambda: r_copy(b, m).start())

    def down_ready(b):
        down_own(b).wait()
        down_push(b).wait_recv()

    before = second = order(L - 2)

    def group_tiles(m, act):
        first = flip(g, m, G) * cap

        @pl.loop(0, cap // tile)
        def _(t):
            act(pl.ds(pl.multiple_of(first + t * tile, 16), tile))

    def add_before(at):
        both = gate_up(before, (L - 2) % 2, at)
        for i in range(2):
            acc[i, at] += both[i]

    def hide(at):
        both = gate_up(last, (L - 1) % 2, at)
        both = [both[i] + acc[i, at] for i in range(2)]
        half = 0.5 * both[0]
        hbuf[core, at] = ((half + half * jnp.tanh(half)) * both[1]).astype(BF16)

    def take_before(m):
        d_copy(before, m).wait_recv()
        group_tiles(m, add_before)

    def close(m):
        d_copy(last, m).wait_recv()
        group_tiles(m, hide)
        h_copy(m).start()

    def send_first(m):
        h_copy(m).wait_recv()
        project(0, m)
        r_copy(last, m).start()

    build_mix(L - 3)

    @pl.loop(1, G)
    def _(m):
        e_copy(before, m).wait_recv()
        d_copy(before, m).start()

    for s in (L - 2, L - 1):
        for i in range(2):
            w_load(s, i).wait()
    down_ready(last)

    @pl.loop(0, far)
    def _(m):
        take_before(m)
        pl.when(m == 0)(lambda: close(0))

        @pl.when(m == 1)
        def _():
            @pl.loop(1, far)
            def _(k):
                e_copy(last, k).wait_recv()
                d_copy(last, k).start()

    @pl.loop(1, G)
    def _(m):
        @pl.when(m == far)
        def _():
            @pl.when(jnp.logical_not(next_to_end))
            def _():
                e_copy(last, far).wait_recv()

            d_copy(last, far).start()
            send_first(far - 1)
            take_before(far)

        close(m)
        pl.when(jnp.logical_and(m > 1, m < far))(lambda: send_first(m - 1))

    down_ready(second)

    @pl.loop(1, far)
    def _(m):
        project(1, m)

    h_copy(far).wait_recv()

    @pl.loop(0, 2)
    def _(i):
        project(1 - i, far)

        @pl.when(i == 0)
        def _():
            pl.when(sent(second, far))(lambda: add_extra(second, tbuf))
            pl.when(jnp.logical_not(inside))(lambda: wait_sends(0))
            start_sends(1)

    h_copy(0).wait_recv()

    @pl.loop(0, 2)
    def _(i):
        project(i, 0)

    @pl.when(jnp.logical_not(jnp.logical_or(skipped(last), next_to_end)))
    def _():
        obuf[last, far - 1] = ebuf[...].astype(BF16)
        r_copy(last, far).start()

    build_mix(L - 2)

    pl.when(z < L - 1)(z_copy(z, 0).wait_send)
    pl.when(z > 0)(z_copy(z, 1).wait_send)
    pl.when(next_to_end)(l_copy().wait_send)

    @pl.loop(0, L)
    def _(b):
        pl.when(jnp.logical_and(b < z, z < L - 1))(z_copy(b, 0).wait_send)
        pl.when(jnp.logical_and(b > z, z > 0))(z_copy(b, 1).wait_send)

        @pl.when(skipped(b))
        def _():
            rbuf[b, group_rows(flip(g, far, G))] = jnp.zeros((cap, cols), BF16)

    def combined(b, t):
        parts = []
        for k in range(blocks):
            c, l, first = mix_place(k)
            parts.append(piece[c, l, pl.ds(pl.multiple_of(first + t * step, 16), step)])
        return jnp.dot(jnp.concatenate(parts, axis=1), rbuf[b], preferred_element_type=F32)

    def arrived(b):
        @pl.loop(1, G)
        def _(m):
            @pl.when(jnp.logical_not(jnp.logical_and(m == far, skipped(b))))
            def _():
                r_copy(b, m).wait_recv()

    def combine(i):
        b = order(L - 1 - i)
        more = jnp.where(b > z, z, L - 1 - z) > 0
        arrived(b)

        @pl.loop(0, tiles)
        def _(t):
            at = rows_of(t)
            value = combined(b, t)

            @pl.when(more)
            def _():
                y_wait(b, t)
                zbuf[b, at] = (value + rin[b, at].astype(F32)).astype(BF16)

            @pl.when(jnp.logical_not(more))
            def _():
                zbuf[b, at] = value.astype(BF16)

            pl.when(b > z)(y_copy(b, 0, t).start)
            pl.when(b < z)(y_copy(b, 1, t).start)

    @pl.loop(1, L)
    def _(i):
        b = order(L - 1 - i)

        @pl.when(i > 1)
        def _():
            down_ready(b)

            @pl.loop(0, far)
            def _(j):
                project(i, far - j)

            @pl.when(jnp.logical_and(next_to_end, i == 2))
            def _():
                add_extra(last, ebuf)
                r_copy(last, far).start()

            pl.when(sent(b, far))(lambda: add_extra(b, tbuf))

            wait_sends(i - 1)

            start_sends(i)

            project(i, 0)

        late = jnp.where(inside, 2, 1)
        pl.when(i >= late)(lambda: combine(i - late))

    pl.when(inside)(lambda: combine(L - 2))
    arrived(z)

    @pl.loop(0, tiles)
    def _(t):
        tbuf[rows_of(t)] = combined(z, t)

    @pl.loop(0, tiles)
    def _(t):
        at = rows_of(t)
        for side, slot in ((0, z), (1, L)):
            @pl.when(z > 0 if side == 0 else z < L - 1)
            def _():
                y_wait(slot, t)
                tbuf[at] += rin[slot, at].astype(F32)

    def out_copy(t):
        at = slice(t * step, (t + 1) * step)
        return pltpu.make_async_copy(nbuf.at[at], out_ref.at[at], xs.at[t])

    stat2[me] = squares_of(tbuf[...], nb)
    for k in range(1, n):
        stat_copy(stat2, ts, tr, k).start()
    post = post_ref[...].astype(F32).reshape(1, cols)
    scol[...] = row_scale(stat2, ts, tr)
    for r in range(nb):
        at = slice(r * LANES, (r + 1) * LANES)
        nbuf[at] = (tbuf[at] * scol[:, r : r + 1] * post).astype(BF16)
        if (r + 1) * LANES % step == 0:
            out_copy(r * LANES // step).start()

    for k in range(1, n):
        stat_copy(stat, ss, sr, k).wait_send()
        stat_copy(stat2, ts, tr, k).wait_send()

    pl.when(z == 0)(a_copy(farthest, 0).wait_send)
    pl.when(z == L - 1)(a_copy(farthest, 1).wait_send)

    @pl.when(inside)
    def _():
        a_copy(z + 1, 0).wait_send()
        a_copy(z - 1, 1).wait_send()

    pl.when(inside)(lambda: wait_sends(0))
    wait_sends(L - 1)

    @pl.loop(0, L)
    def _(b):
        down_push(b).wait_send()

        @pl.loop(0, tiles)
        def _(t):
            pl.when(b > z)(y_copy(b, 0, t).wait_send)
            pl.when(b < z)(y_copy(b, 1, t).wait_send)

    @pl.loop(0, G)
    def _(m):
        d_copy(last, m).wait_send()

    @pl.loop(0, G)
    def _(m):
        h_copy(m).wait_send()

    for t in range(tiles):
        out_copy(t).wait()


def on_device(
    tokens, pre_gain, route_ids, route_weights, gate_weight, up_weight, down_weight, post_gain
):
    tok, cols = tokens.shape
    top = route_ids.shape[1]
    G = lax.axis_size("ep")
    n = lax.axis_size("tp")
    L = n // 2
    cap = 9 * tok * top // (8 * G)
    rows = G * cap
    units = gate_weight.shape[2]
    nb = tok // LANES
    tile = cap
    tiles = tok // min(256, tok)
    vmem = pl.BlockSpec(memory_space=pltpu.VMEM)
    hbm = pl.BlockSpec(memory_space=pl.ANY)
    return pl.pallas_call(
        functools.partial(layer_kernel, L, G, cap, tile),
        out_shape=jax.ShapeDtypeStruct((tok, cols), BF16),
        in_specs=[hbm] + [vmem] * 4 + [hbm] * 3,
        out_specs=hbm,
        scratch_shapes=[
            pltpu.VMEM((L, tok, cols), BF16),
            pltpu.VMEM((tok, cols), BF16),
            pltpu.VMEM((L, G - 1, cap, cols), BF16),
            pltpu.VMEM((2, L, rows, cols), BF16),
            pltpu.VMEM((2, 2, 2 * cols, units), BF16),
            pltpu.VMEM((2, rows, units), F32),
            pltpu.VMEM((2, rows, units), BF16),
            pltpu.VMEM((L, 2 * units, cols), BF16),
            pltpu.VMEM((L, rows, cols), BF16),
            pltpu.VMEM((L + 1, tok, cols), BF16),
            pltpu.VMEM((2, cap, cols), BF16),
            pltpu.VMEM((cap, cols), F32),
            pltpu.VMEM((tok, cols), F32),
            pltpu.VMEM((n, 2 * nb, LANES), F32),
            pltpu.VMEM((n, nb, LANES), F32),
            pltpu.VMEM((G * nb, LANES), jnp.int32),
            pltpu.VMEM((LANES, LANES), jnp.int32),
            pltpu.VMEM((LANES, LANES), F32),
            pltpu.VMEM((LANES, LANES), F32),
            DMA((2, L)), DMA((L,)),
            DMA((L, G)), DMA((L, G)),
            DMA((3,)),
            DMA((L, G)), DMA((L, G)),
            DMA((2, 2)),
            DMA((L,)), DMA((L,)), DMA((L,)),
            DMA((G,)), DMA((G,)),
            DMA((L, G)), DMA((L, G)),
            DMA((2,)), DMA((2,)),
            DMA((L, tiles)), DMA((L + 1, tiles)),
            DMA((n,)), DMA((n,)),
            DMA((n,)), DMA((n,)),
            DMA((tiles,)),
        ],
        compiler_params=pltpu.CompilerParams(
            collective_id=1, has_side_effects=True, vmem_limit_bytes=62 * 2**20
        ),
        name="layer",
    )(
        tokens, pre_gain, post_gain, route_ids.T, route_weights.T,
        gate_weight[0], up_weight[0], down_weight[0],
    )


def solution(mesh):
    placed = (
        P("ep", "tp"),
        P("tp"),
        P("ep", None),
        P("ep", None),
        P("ep", None, "tp"),
        P("ep", None, "tp"),
        P("ep", "tp", None),
        P("tp"),
    )
    return jax.shard_map(
        on_device, mesh=mesh, in_specs=placed, out_specs=P("ep", "tp"), check_vma=False
    )
```

```python
import functools

import jax
import jax.numpy as jnp
from jax import lax
from jax.experimental import pallas as pl
from jax.experimental.pallas import tpu as pltpu
from jax.sharding import PartitionSpec as P

epsilon = 1e-06
MESH = pl.DeviceIdType.MESH
DMA = pltpu.SemaphoreType.DMA
BF16 = jnp.bfloat16
F32 = jnp.float32
LANES = 128


def flip(a, m, size):
    total, bit = 0, 1
    while bit < size:
        total = total + (((a // bit) % 2 + (m // bit) % 2) % 2) * bit
        bit *= 2
    return total


def columns_of(values):
    rows = values.shape[0]
    if rows < LANES:
        values = jnp.concatenate([values, jnp.zeros((LANES - rows, LANES), values.dtype)], axis=0)
    return values.T


def fold(wide, nb):
    row = lax.broadcasted_iota(jnp.int32, (nb, LANES), 0)
    total = None
    for r in range(nb):
        part = jnp.broadcast_to(wide[:, r * LANES : (r + 1) * LANES], (nb, LANES))
        total = part if total is None else jnp.where(row == r, part, total)
    return total


def squares_of(v, nb):
    square = v * v
    high = square.astype(BF16)
    low = (square - high.astype(F32)).astype(BF16)
    ones = jnp.ones((nb, v.shape[1]), BF16)
    dims = (((1,), (1,)), ((), ()))
    wide = lax.dot_general(ones, high, dims, preferred_element_type=F32)
    wide += lax.dot_general(ones, low, dims, preferred_element_type=F32)
    return fold(wide, nb)


def layer_kernel(
    L, G, cap, tile,
    x_ref, pre_ref, post_ref, ids_ref, rw_ref, gate_ref, up_ref, down_ref, out_ref,
    zbuf, nbuf, obuf, piece, wbuf, acc, hbuf, dbuf, rbuf, rin, abuf, ebuf, tbuf,
    stat, stat2, kbuf, kcol, wcol, scol,
    zs, zr, es, er, fs, ds, dr, ws, dl, dps, dpr, hs, hr, rs, rr, as_, ar, ys, yr, ss, sr, ts, tr, xs,
):
    tok, cols = nbuf.shape
    nb = tok // LANES
    n = 2 * L
    units = gate_ref.shape[1]
    rows = G * cap
    far = G - 1
    me, g = lax.axis_index("tp"), lax.axis_index("ep")
    core, z = lax.rem(me, 2), me // 2
    partner = {"tp": me + 1 - 2 * core}
    inside = jnp.logical_and(z > 0, z < L - 1)
    inner = jnp.minimum(z, L - 1 - z)
    width = n * cols
    step = min(256, tok)
    tiles = tok // step

    def order(s):
        near = jnp.where(s % 2 == 1, z - (s + 1) // 2, z + (s + 1) // 2)
        rest = jnp.where(2 * z > L - 1, z - (s - inner), z + (s - inner))
        return jnp.where(s <= 2 * inner, near, rest)

    farthest = jnp.where(2 * z > L - 1, 0, L - 1)
    last = order(L - 1)
    end_left = z == 1
    next_to_end = jnp.logical_or(z == 1, z == L - 2)

    def skipped(b):
        beside = jnp.logical_or(b == z + 1, b == z - 1)
        return jnp.where(inside, beside, b == farthest)

    def group_rows(e):
        return pl.ds(pl.multiple_of(e * cap, 16), cap)

    def remote(src, dst, send, recv, to):
        return pltpu.make_async_remote_copy(
            src_ref=src, dst_ref=dst, send_sem=send, recv_sem=recv, device_id=to, device_id_type=MESH
        )

    def at_z(to):
        return {"tp": to * 2 + core}

    def at_g(m):
        return {"ep": flip(g, m, G)}

    def w_load(s, i):
        ref = (gate_ref, up_ref)[i]
        depth = pl.ds(pl.multiple_of(order(s) * 2 * cols, LANES), 2 * cols)
        return pltpu.make_async_copy(ref.at[depth], wbuf.at[s % 2, i], ws.at[s % 2, i])

    def my_units(c):
        return pl.ds(pl.multiple_of(c * units, 16), units)

    def down_part(b, c):
        return down_ref.at[:, pl.ds(pl.multiple_of((b * 2 + c) * cols, LANES), cols)]

    def down_own(b):
        return pltpu.make_async_copy(down_part(b, core), dbuf.at[b, my_units(core)], dl.at[b])

    def down_push(b):
        return remote(
            down_part(b, 1 - core), dbuf.at[b, my_units(core)], dps.at[b], dpr.at[b], partner
        )

    def z_copy(b, side):
        return remote(zbuf.at[b], zbuf.at[b], zs.at[side, b], zr.at[b], at_z(z + 1 - 2 * side))

    def e_copy(b, m):
        return remote(
            obuf.at[b, m - 1], piece.at[core, b, group_rows(g)], es.at[b, m], er.at[b, m], at_g(m)
        )

    def f_copy(side):
        area = piece.at[core, z, group_rows(flip(g, far, G))]
        return remote(area, area, fs.at[side], er.at[z, far], at_z(z + 1 - 2 * side))

    def l_copy():
        area = piece.at[core, farthest, group_rows(flip(g, far, G))]
        return remote(area, area, fs.at[2], er.at[farthest, far], at_z(jnp.where(end_left, 0, L - 1)))

    def d_copy(b, m):
        area = piece.at[core, b, group_rows(flip(g, m, G))]
        return remote(area, area, ds.at[b, m], dr.at[b, m], partner)

    half = cap // 2 if cap % 32 == 0 else cap

    def h_copy(m, t):
        at = pl.ds(pl.multiple_of(flip(g, m, G) * cap + t * half, 16), half)
        area = hbuf.at[core, at]
        return remote(area, area, hs.at[m, t], hr.at[m, t], partner)

    def h_wait(m):
        for t in range(cap // half):
            h_copy(m, t).wait_recv()

    def r_copy(b, m):
        return remote(
            obuf.at[b, m - 1], rbuf.at[b, group_rows(g)], rs.at[b, m], rr.at[b, m], at_g(m)
        )

    def a_copy(b, side):
        return remote(obuf.at[b, far - 1], abuf.at[side], as_.at[side], ar.at[side], at_z(z + 1 - 2 * side))

    def rows_of(t):
        return pl.ds(pl.multiple_of(t * step, 16), step)

    def y_copy(b, side, t):
        to = z + 1 - 2 * side
        slot = jnp.where(jnp.logical_and(to == b, side == 1), L, b)
        return remote(zbuf.at[b, rows_of(t)], rin.at[slot, rows_of(t)], ys.at[b, t], yr.at[slot, t], at_z(to))

    def y_wait(slot, t):
        area = rin.at[slot, rows_of(t)]
        remote(area, area, ys.at[0, t], yr.at[slot, t], partner).wait_recv()

    def stat_copy(buf, send, recv, k):
        to = lax.rem(me + k, n)
        return remote(buf.at[me], buf.at[me], send.at[to], recv.at[me], {"tp": to})

    def stat_wait(buf, send, recv, k):
        of = lax.rem(me + n - k, n)
        remote(buf.at[of], buf.at[of], send.at[of], recv.at[of], {"tp": of}).wait_recv()

    barrier = pltpu.get_barrier_semaphore()
    for k in range(1, n):
        pl.semaphore_signal(barrier, inc=1, device_id={"tp": lax.rem(me + k, n)}, device_id_type=MESH)
    for m in range(1, G):
        pl.semaphore_signal(barrier, inc=1, device_id=at_g(m), device_id_type=MESH)
    x_load = pltpu.make_async_copy(x_ref, zbuf.at[z], xs.at[0])
    x_load.start()
    for s in range(2):
        for i in range(2):
            w_load(s, i).start()

    @pl.loop(0, L)
    def _(b):
        down_own(b).start()

    x_load.wait()
    stat[me, 0:nb] = squares_of(zbuf[z].astype(F32), nb)
    pre = pre_ref[...].astype(F32).reshape(1, cols)
    for c in range(cols // LANES):
        stat[me, nb + c : nb + c + 1] = pre[:, c * LANES : (c + 1) * LANES]

    pl.semaphore_wait(barrier, n + G - 2)
    for k in range(1, n):
        stat_copy(stat, ss, sr, k).start()
    pl.when(z < L - 1)(z_copy(z, 0).start)
    pl.when(z > 0)(z_copy(z, 1).start)

    ids, weights = ids_ref[...], rw_ref[...]
    top = ids.shape[0]
    id_rows = [fold(ids[t : t + 1], nb) for t in range(top)]
    weight_rows = [fold(weights[t : t + 1], nb) for t in range(top)]
    members, shares = [], []
    for e in range(G):
        named = [r == e for r in id_rows]
        members.append(sum(jnp.where(q, 1.0, 0.0) for q in named))
        shares.append(sum(jnp.where(q, w, 0.0) for q, w in zip(named, weight_rows)))
    member = jnp.concatenate(members, axis=0)
    small = member.astype(BF16)
    lane_a = lax.broadcasted_iota(jnp.int32, (LANES, LANES), 0)
    lane_b = lax.broadcasted_iota(jnp.int32, (LANES, LANES), 1)
    both = jnp.concatenate(
        [jnp.where(lane_a < lane_b, 1.0, 0.0).astype(BF16), jnp.ones((LANES, LANES), BF16)], axis=1
    )
    counted = jnp.dot(small, both, preferred_element_type=F32)
    row_a = lax.broadcasted_iota(jnp.int32, (G * nb, G * nb), 0)
    row_b = lax.broadcasted_iota(jnp.int32, (G * nb, G * nb), 1)
    ahead = jnp.where(jnp.logical_and(row_a // nb == row_b // nb, row_b < row_a), 1.0, 0.0).astype(BF16)
    rank = counted[:, :LANES] + jnp.dot(
        ahead, counted[:, LANES:].astype(BF16), preferred_element_type=F32
    )
    base = (lax.broadcasted_iota(jnp.int32, (G * nb, LANES), 0) // nb * cap).astype(F32)
    key = jnp.where(member > 0.5, rank + base, -1.0)
    kbuf[...] = key.astype(jnp.int32)
    kcol[...] = columns_of(key).astype(jnp.int32)
    wcol[...] = columns_of(jnp.concatenate(shares, axis=0))

    for e in range(G):
        wanted = lax.broadcasted_iota(jnp.int32, (cap, LANES), 0) + e * cap
        for r in range(nb):
            l, lane = r * LANES // cols, r * LANES % cols
            rbuf[l, e * cap : (e + 1) * cap, lane : lane + LANES] = jnp.where(
                kbuf[e * nb + r : e * nb + r + 1] == wanted, 1.0, 0.0
            ).astype(BF16)

    def row_scale(buf, send, recv):
        for k in range(1, n):
            stat_wait(buf, send, recv, k)
        total = buf[0, 0:nb]
        for k in range(1, n):
            total = total + buf[k, 0:nb]
        return columns_of(lax.rsqrt(total / width + epsilon))

    scol[...] = row_scale(stat, ss, sr)

    @pl.loop(0, L)
    def _(b):
        down_push(b).start()

    def take(s):
        b = order(s)
        z_copy(b, 0).wait_recv()
        pl.when(jnp.logical_and(b < z, z < L - 1))(z_copy(b, 0).start)
        pl.when(jnp.logical_and(b > z, z > 0))(z_copy(b, 1).start)

    def process(s):
        b = order(s)
        gain = jnp.concatenate(
            [stat[b * 2 + core, nb + c : nb + c + 1] for c in range(cols // LANES)], axis=1
        )
        for r in range(nb):
            at = slice(r * LANES, (r + 1) * LANES)
            nbuf[at] = (zbuf[b, at].astype(F32) * scol[:, r : r + 1] * gain).astype(BF16)

        @pl.loop(0, G)
        def _(j):
            m = G - 1 - j

            @pl.when(jnp.logical_not(jnp.logical_and(m == far, skipped(b))))
            def _():
                at = group_rows(flip(g, m, G))
                chooser = jnp.concatenate([rbuf[l, at] for l in range(tok // cols)], axis=1)
                chosen = jnp.dot(chooser, nbuf[...], preferred_element_type=F32).astype(BF16)

                @pl.when(m > 0)
                def _():
                    obuf[b, m - 1] = chosen
                    e_copy(b, m).start()

                @pl.when(m == 0)
                def _():
                    piece[core, b, group_rows(g)] = chosen
                    d_copy(b, 0).start()

    def gate_up(b, slot, at):
        left = jnp.concatenate([piece[0, b, at], piece[1, b, at]], axis=1)
        return [jnp.dot(left, wbuf[slot, i], preferred_element_type=F32) for i in range(2)]

    per = rows // tok
    blocks = rows // cols

    def mix_place(k):
        return k // per % 2, order(k // (2 * per)), (k % per) * tok

    def build_mix(q):
        b = order(q)

        @pl.loop(0, G)
        def _(m):
            d_copy(b, m).wait_send()

        if q == 0:
            pl.when(z < L - 2)(f_copy(0).wait_send)
            pl.when(z > 1)(f_copy(1).wait_send)
        for k in range(2 * per * q, min(2 * per * (q + 1), blocks)):
            c, b, first = mix_place(k)
            lane = lax.broadcasted_iota(jnp.int32, (LANES, cols), 1) + k * cols
            for r in range(nb):
                value = jnp.zeros((LANES, cols), F32)
                for e in range(k * cols // cap, ((k + 1) * cols - 1) // cap + 1):
                    p = e * nb + r
                    value = jnp.where(kcol[:, p : p + 1] == lane, wcol[:, p : p + 1], value)
                piece[c, b, first + r * LANES : first + (r + 1) * LANES] = value.astype(BF16)

    def finish(s):
        b, slot = order(s), s % 2

        for q in range(L - 3):
            pl.when(s == q + 1)(functools.partial(build_mix, q))

        @pl.loop(1, G)
        def _(j):
            m = G - j
            e_copy(b, m).wait_recv()

            @pl.when(jnp.logical_and(m == far, b == z))
            def _():
                pl.when(z < L - 2)(f_copy(0).start)
                pl.when(z > 1)(f_copy(1).start)

            d_copy(b, m).start()

        @pl.loop(0, G)
        def _(m):
            d_copy(b, m).wait_recv()

        for i in range(2):
            w_load(s, i).wait()

        @pl.loop(0, rows // tile)
        def _(t):
            at = pl.ds(pl.multiple_of(t * tile, 16), tile)
            both = gate_up(b, slot, at)

            @pl.when(s == 0)
            def _():
                for i in range(2):
                    acc[i, at] = both[i]

            @pl.when(s > 0)
            def _():
                for i in range(2):
                    acc[i, at] += both[i]

        @pl.when(s + 2 < L)
        def _():
            for i in range(2):
                w_load(s + 2, i).start()

    @pl.loop(0, L)
    def _(s):
        early = jnp.logical_and(inside, s > 0)
        low = jnp.where(jnp.logical_and(early, s > 1), s + 1, s)
        high = jnp.where(early, jnp.minimum(s + 2, L), s + 1)

        @pl.when(s > 0)
        def _():
            pl.loop(low, high)(take)

        pl.loop(low, high)(process)

        @pl.when(jnp.logical_and(next_to_end, s == L - 1))
        def _():
            e_copy(farthest, far).wait_recv()
            l_copy().start()

        pl.when(jnp.logical_and(s > 0, s < L - 1))(lambda: finish(s - 1))

    def extra(b, side):
        if side == 0:
            return jnp.logical_and(z > 0, b == jnp.where(z > 1, z, L - 1))
        return jnp.logical_and(z < L - 1, b == jnp.where(z < L - 2, z, 0))

    def add_extra(b, held):
        for side in range(2):
            @pl.when(extra(b, side))
            def _():
                a_copy(b, side).wait_recv()
                held[0:cap] += abuf[side].astype(F32)

        obuf[b, far - 1] = held[0:cap].astype(BF16)

    def project(i, m):
        b = order(L - 1 - i)
        at = group_rows(flip(g, m, G))
        if units % LANES == 0:
            left = jnp.concatenate([hbuf[0, at], hbuf[1, at]], axis=1)
            result = jnp.dot(left, dbuf[b], preferred_element_type=F32)
        else:
            result = jnp.dot(hbuf[0, at], dbuf[b, 0:units], preferred_element_type=F32)
            result += jnp.dot(hbuf[1, at], dbuf[b, units:], preferred_element_type=F32)

        @pl.when(m == 0)
        def _():
            rbuf[b, at] = result.astype(BF16)

        @pl.when(jnp.logical_and(m > 0, m < far))
        def _():
            e_copy(b, m).wait_send()
            obuf[b, m - 1] = result.astype(BF16)

        @pl.when(m == far)
        def _():
            @pl.when(skipped(b))
            def _():
                obuf[b, far - 1] = result.astype(BF16)
                to_right = jnp.where(inside, b > z, z == 0)
                pl.when(to_right)(a_copy(b, 0).start)
                pl.when(jnp.logical_not(to_right))(a_copy(b, 1).start)

            @pl.when(jnp.logical_not(skipped(b)))
            def _():
                e_copy(b, far).wait_send()

                @pl.when(i > 0)
                def _():
                    tbuf[0:cap] = result

                @pl.when(i == 0)
                def _():
                    ebuf[...] = result

    def sent(b, m):
        return jnp.logical_not(jnp.logical_and(m == far, skipped(b)))

    def wait_sends(i):
        b = order(L - 1 - i)

        @pl.loop(1, G)
        def _(m):
            pl.when(sent(b, m))(lambda: r_copy(b, m).wait_send())

    def start_sends(b):
        @pl.loop(0, far)
        def _(j):
            m = far - j
            pl.when(sent(b, m))(lambda: r_copy(b, m).start())

    def down_ready(b):
        down_own(b).wait()
        down_push(b).wait_recv()

    before = second = order(L - 2)

    def take_before(m):
        d_copy(before, m).wait_recv()
        at = group_rows(flip(g, m, G))
        both = gate_up(before, (L - 2) % 2, at)
        for i in range(2):
            acc[i, at] += both[i]

    def close(m):
        d_copy(last, m).wait_recv()

        @pl.loop(0, cap // half)
        def _(t):
            at = pl.ds(pl.multiple_of(flip(g, m, G) * cap + t * half, 16), half)
            both = gate_up(last, (L - 1) % 2, at)
            gates = 0.5 * (both[0] + acc[0, at])
            hbuf[core, at] = ((gates + gates * jnp.tanh(gates)) * (both[1] + acc[1, at])).astype(BF16)
            h_copy(m, t).start()

    build_mix(L - 3)

    @pl.loop(1, G)
    def _(m):
        e_copy(before, m).wait_recv()
        d_copy(before, m).start()

    for s in (L - 2, L - 1):
        for i in range(2):
            w_load(s, i).wait()
    down_ready(last)
    down_ready(second)

    @pl.loop(0, 2 * far + 1)
    def _(v):
        u = v - far
        pl.when(jnp.logical_or(v < far, u == far))(lambda: take_before(jnp.minimum(v, far)))

        @pl.when(v == 1)
        def _():
            @pl.loop(1, far)
            def _(k):
                e_copy(last, k).wait_recv()
                d_copy(last, k).start()

        @pl.when(u == far - 1)
        def _():
            @pl.when(jnp.logical_not(next_to_end))
            def _():
                e_copy(last, far).wait_recv()

            d_copy(last, far).start()

        @pl.when(jnp.logical_or(v == 0, jnp.logical_and(u >= 0, u != far - 1)))
        def _():
            close(jnp.where(v == 0, 0, jnp.minimum(u + 1, far)))

        @pl.when(jnp.logical_and(u > 0, u < far))
        def _():
            h_wait(u)
            project(0, u)
            r_copy(last, u).start()

    def first_far():
        obuf[last, far - 1] = ebuf[...].astype(BF16)
        r_copy(last, far).start()

    def after_dispatch():
        build_mix(L - 2)
        pl.when(z < L - 1)(z_copy(z, 0).wait_send)
        pl.when(z > 0)(z_copy(z, 1).wait_send)
        pl.when(next_to_end)(l_copy().wait_send)

        @pl.loop(0, L)
        def _(b):
            pl.when(jnp.logical_and(b < z, z < L - 1))(z_copy(b, 0).wait_send)
            pl.when(jnp.logical_and(b > z, z > 0))(z_copy(b, 1).wait_send)

            @pl.when(skipped(b))
            def _():
                rbuf[b, group_rows(flip(g, far, G))] = jnp.zeros((cap, cols), BF16)

    def combined(b, t):
        parts = []
        for k in range(blocks):
            c, l, first = mix_place(k)
            parts.append(piece[c, l, pl.ds(pl.multiple_of(first + t * step, 16), step)])
        return jnp.dot(jnp.concatenate(parts, axis=1), rbuf[b], preferred_element_type=F32)

    def arrived(b):
        @pl.loop(1, G)
        def _(m):
            @pl.when(jnp.logical_not(jnp.logical_and(m == far, skipped(b))))
            def _():
                r_copy(b, m).wait_recv()

    def combine(i):
        b = order(L - 1 - i)
        own = b == z
        more = jnp.logical_and(jnp.logical_not(own), jnp.where(b > z, z, L - 1 - z) > 0)
        ends_here = jnp.logical_or(own, more)
        arrived(b)

        @pl.loop(0, tiles)
        def _(t):
            at = rows_of(t)
            value = combined(b, t)

            @pl.when(own)
            def _():
                tbuf[at] = value

            @pl.when(more)
            def _():
                y_wait(b, t)
                zbuf[b, at] = (value + rin[b, at].astype(F32)).astype(BF16)

            @pl.when(jnp.logical_not(ends_here))
            def _():
                zbuf[b, at] = value.astype(BF16)

            pl.when(b > z)(y_copy(b, 0, t).start)
            pl.when(b < z)(y_copy(b, 1, t).start)

    def launch(i):
        b = order(L - 1 - i)

        @pl.when(jnp.logical_and(next_to_end, i == 2))
        def _():
            add_extra(last, ebuf)
            r_copy(last, far).start()

        pl.when(sent(b, far))(lambda: add_extra(b, tbuf))
        pl.when(jnp.logical_or(i > 1, jnp.logical_not(inside)))(lambda: wait_sends(i - 1))
        start_sends(b)

    late = jnp.where(inside, 2, 1)

    @pl.loop(1, L + 2)
    def _(i):
        first = i == 1

        @pl.when(i < L)
        def _():
            pl.when(i > 1)(lambda: down_ready(order(L - 1 - i)))

            @pl.loop(0, jnp.where(first, G + 2, G))
            def _(j):
                pl.when(jnp.logical_and(first, j == far - 1))(lambda: h_wait(far))
                pl.when(jnp.logical_and(first, j == far + 1))(lambda: h_wait(0))
                m = jnp.where(first, jnp.where(j < far, j + 1, jnp.where(j == far, far, 0)), far - j)
                rest = jnp.logical_and(first, jnp.logical_or(j == far, j == far + 1))
                project(jnp.where(rest, 0, i), m)
                pl.when(j == far - 1)(lambda: launch(i))

        @pl.when(first)
        def _():
            pl.when(jnp.logical_not(jnp.logical_or(skipped(last), next_to_end)))(first_far)
            after_dispatch()

        c = i - late
        pl.when(jnp.logical_and(c >= 0, c < L))(lambda: combine(c))

    @pl.loop(0, tiles)
    def _(t):
        at = rows_of(t)
        for side, slot in ((0, z), (1, L)):
            @pl.when(z > 0 if side == 0 else z < L - 1)
            def _():
                y_wait(slot, t)
                tbuf[at] += rin[slot, at].astype(F32)

    def out_copy(t):
        at = slice(t * step, (t + 1) * step)
        return pltpu.make_async_copy(nbuf.at[at], out_ref.at[at], xs.at[t])

    stat2[me] = squares_of(tbuf[...], nb)
    for k in range(1, n):
        stat_copy(stat2, ts, tr, k).start()
    for k in range(1, n):
        stat_copy(stat, ss, sr, k).wait_send()

    pl.when(z == 0)(a_copy(farthest, 0).wait_send)
    pl.when(z == L - 1)(a_copy(farthest, 1).wait_send)

    @pl.when(inside)
    def _():
        a_copy(z + 1, 0).wait_send()
        a_copy(z - 1, 1).wait_send()

    pl.when(inside)(lambda: wait_sends(0))
    wait_sends(L - 1)

    @pl.loop(0, L)
    def _(b):
        down_push(b).wait_send()

        @pl.loop(0, tiles)
        def _(t):
            pl.when(b > z)(y_copy(b, 0, t).wait_send)
            pl.when(b < z)(y_copy(b, 1, t).wait_send)

    @pl.loop(0, G)
    def _(m):
        d_copy(last, m).wait_send()

    @pl.loop(0, G)
    def _(m):
        for t in range(cap // half):
            h_copy(m, t).wait_send()

    post = post_ref[...].astype(F32).reshape(1, cols)
    scol[...] = row_scale(stat2, ts, tr)
    for r in range(nb):
        at = slice(r * LANES, (r + 1) * LANES)
        nbuf[at] = (tbuf[at] * scol[:, r : r + 1] * post).astype(BF16)
        if (r + 1) * LANES % step == 0:
            out_copy(r * LANES // step).start()

    for k in range(1, n):
        stat_copy(stat2, ts, tr, k).wait_send()
    for t in range(tiles):
        out_copy(t).wait()


def on_device(
    tokens, pre_gain, route_ids, route_weights, gate_weight, up_weight, down_weight, post_gain
):
    tok, cols = tokens.shape
    top = route_ids.shape[1]
    G = lax.axis_size("ep")
    n = lax.axis_size("tp")
    L = n // 2
    cap = 9 * tok * top // (8 * G)
    rows = G * cap
    units = gate_weight.shape[2]
    nb = tok // LANES
    tile = cap
    tiles = tok // min(256, tok)
    vmem = pl.BlockSpec(memory_space=pltpu.VMEM)
    hbm = pl.BlockSpec(memory_space=pl.ANY)
    return pl.pallas_call(
        functools.partial(layer_kernel, L, G, cap, tile),
        out_shape=jax.ShapeDtypeStruct((tok, cols), BF16),
        in_specs=[hbm] + [vmem] * 4 + [hbm] * 3,
        out_specs=hbm,
        scratch_shapes=[
            pltpu.VMEM((L, tok, cols), BF16),
            pltpu.VMEM((tok, cols), BF16),
            pltpu.VMEM((L, G - 1, cap, cols), BF16),
            pltpu.VMEM((2, L, rows, cols), BF16),
            pltpu.VMEM((2, 2, 2 * cols, units), BF16),
            pltpu.VMEM((2, rows, units), F32),
            pltpu.VMEM((2, rows, units), BF16),
            pltpu.VMEM((L, 2 * units, cols), BF16),
            pltpu.VMEM((L, rows, cols), BF16),
            pltpu.VMEM((L + 1, tok, cols), BF16),
            pltpu.VMEM((2, cap, cols), BF16),
            pltpu.VMEM((cap, cols), F32),
            pltpu.VMEM((tok, cols), F32),
            pltpu.VMEM((n, 2 * nb, LANES), F32),
            pltpu.VMEM((n, nb, LANES), F32),
            pltpu.VMEM((G * nb, LANES), jnp.int32),
            pltpu.VMEM((LANES, LANES), jnp.int32),
            pltpu.VMEM((LANES, LANES), F32),
            pltpu.VMEM((LANES, LANES), F32),
            DMA((2, L)), DMA((L,)),
            DMA((L, G)), DMA((L, G)),
            DMA((3,)),
            DMA((L, G)), DMA((L, G)),
            DMA((2, 2)),
            DMA((L,)), DMA((L,)), DMA((L,)),
            DMA((G, 2)), DMA((G, 2)),
            DMA((L, G)), DMA((L, G)),
            DMA((2,)), DMA((2,)),
            DMA((L, tiles)), DMA((L + 1, tiles)),
            DMA((n,)), DMA((n,)),
            DMA((n,)), DMA((n,)),
            DMA((tiles,)),
        ],
        compiler_params=pltpu.CompilerParams(
            collective_id=1, has_side_effects=True, vmem_limit_bytes=62 * 2**20
        ),
        name="layer",
    )(
        tokens, pre_gain, post_gain, route_ids.T, route_weights.T,
        gate_weight[0], up_weight[0], down_weight[0],
    )


def solution(mesh):
    placed = (
        P("ep", "tp"),
        P("tp"),
        P("ep", None),
        P("ep", None),
        P("ep", None, "tp"),
        P("ep", None, "tp"),
        P("ep", "tp", None),
        P("tp"),
    )
    return jax.shard_map(
        on_device, mesh=mesh, in_specs=placed, out_specs=P("ep", "tp"), check_vma=False
    )
```

```python
import functools

import jax
import jax.numpy as jnp
from jax import lax
from jax.experimental import pallas as pl
from jax.experimental.pallas import tpu as pltpu
from jax.sharding import PartitionSpec as P

epsilon = 1e-06
MESH = pl.DeviceIdType.MESH
DMA = pltpu.SemaphoreType.DMA
BF16 = jnp.bfloat16
F32 = jnp.float32
LANES = 128


def flip(a, m, size):
    total, bit = 0, 1
    while bit < size:
        total = total + (((a // bit) % 2 + (m // bit) % 2) % 2) * bit
        bit *= 2
    return total


def columns_of(values):
    rows = values.shape[0]
    if rows < LANES:
        values = jnp.concatenate([values, jnp.zeros((LANES - rows, LANES), values.dtype)], axis=0)
    return values.T


def fold(wide, nb):
    row = lax.broadcasted_iota(jnp.int32, (nb, LANES), 0)
    total = None
    for r in range(nb):
        part = jnp.broadcast_to(wide[:, r * LANES : (r + 1) * LANES], (nb, LANES))
        total = part if total is None else jnp.where(row == r, part, total)
    return total


def squares_of(v, nb):
    square = v * v
    high = square.astype(BF16)
    low = (square - high.astype(F32)).astype(BF16)
    ones = jnp.ones((nb, v.shape[1]), BF16)
    dims = (((1,), (1,)), ((), ()))
    wide = lax.dot_general(ones, high, dims, preferred_element_type=F32)
    wide += lax.dot_general(ones, low, dims, preferred_element_type=F32)
    return fold(wide, nb)


def layer_kernel(
    L, G, cap, tile,
    x_ref, pre_ref, post_ref, ids_ref, rw_ref, gate_ref, up_ref, down_ref, out_ref,
    zbuf, nbuf, obuf, piece, wbuf, acc, hbuf, dbuf, rbuf, rin, abuf, ebuf, tbuf,
    stat, stat2, kbuf, kcol, wcol, scol,
    zs, zr, es, er, fs, ds, dr, ws, dl, dps, dpr, hs, hr, rr, as_, ar, ys, yr, ss, sr, ts, tr, xs,
):
    tok, cols = nbuf.shape
    nb = tok // LANES
    n = 2 * L
    units = gate_ref.shape[1]
    rows = G * cap
    far = G - 1
    me, g = lax.axis_index("tp"), lax.axis_index("ep")
    core, z = lax.rem(me, 2), me // 2
    partner = {"tp": me + 1 - 2 * core}
    inside = jnp.logical_and(z > 0, z < L - 1)
    inner = jnp.minimum(z, L - 1 - z)
    width = n * cols
    step = min(256, tok)
    tiles = tok // step

    def order(s):
        near = jnp.where(s % 2 == 1, z - (s + 1) // 2, z + (s + 1) // 2)
        rest = jnp.where(2 * z > L - 1, z - (s - inner), z + (s - inner))
        return jnp.where(s <= 2 * inner, near, rest)

    farthest = jnp.where(2 * z > L - 1, 0, L - 1)
    last = order(L - 1)
    end_left = z == 1
    next_to_end = jnp.logical_or(z == 1, z == L - 2)

    def skipped(b):
        beside = jnp.logical_or(b == z + 1, b == z - 1)
        return jnp.where(inside, beside, b == farthest)

    def group_rows(e):
        return pl.ds(pl.multiple_of(e * cap, 16), cap)

    def remote(src, dst, send, recv, to):
        return pltpu.make_async_remote_copy(
            src_ref=src, dst_ref=dst, send_sem=send, recv_sem=recv, device_id=to, device_id_type=MESH
        )

    def at_z(to):
        return {"tp": to * 2 + core}

    def at_g(m):
        return {"ep": flip(g, m, G)}

    def w_load(s, i):
        ref = (gate_ref, up_ref)[i]
        depth = pl.ds(pl.multiple_of(order(s) * 2 * cols, LANES), 2 * cols)
        return pltpu.make_async_copy(ref.at[depth], wbuf.at[s % 2, i], ws.at[s % 2, i])

    def my_units(c):
        return pl.ds(pl.multiple_of(c * units, 16), units)

    def down_part(b, c):
        return down_ref.at[:, pl.ds(pl.multiple_of((b * 2 + c) * cols, LANES), cols)]

    def down_own(b):
        return pltpu.make_async_copy(down_part(b, core), dbuf.at[b, my_units(core)], dl.at[0])

    def down_push(b):
        return remote(
            down_part(b, 1 - core), dbuf.at[b, my_units(core)], dps.at[0], dpr.at[0], partner
        )

    def down_all(send, recv):
        area = dbuf.at[:, my_units(core)]
        return remote(area, area, send.at[0], recv.at[0], partner)

    def z_copy(b, side):
        return remote(zbuf.at[b], zbuf.at[b], zs.at[side, b], zr.at[b], at_z(z + 1 - 2 * side))

    def e_copy(b, m):
        return remote(
            obuf.at[b, m - 1], piece.at[core, b, group_rows(g)], es.at[b, m], er.at[b, m], at_g(m)
        )

    def f_copy(side):
        area = piece.at[core, z, group_rows(flip(g, far, G))]
        return remote(area, area, fs.at[side], er.at[z, far], at_z(z + 1 - 2 * side))

    def l_copy():
        area = piece.at[core, farthest, group_rows(flip(g, far, G))]
        return remote(area, area, fs.at[2], er.at[farthest, far], at_z(jnp.where(end_left, 0, L - 1)))

    def d_copy(b, m):
        area = piece.at[core, b, group_rows(flip(g, m, G))]
        return remote(area, area, ds.at[b], dr.at[b, m], partner)

    half = cap // 2 if cap % 32 == 0 else cap

    def d_sent(b):
        area = piece.at[core, b]
        remote(area, area, ds.at[b], dr.at[b, 0], partner).wait_send()

    def h_copy(m, t):
        at = pl.ds(pl.multiple_of(flip(g, m, G) * cap + t * half, 16), half)
        area = hbuf.at[core, at]
        return remote(area, area, hs.at[m], hr.at[m], partner)

    def h_all(m):
        area = hbuf.at[core, group_rows(flip(g, m, G))]
        return remote(area, area, hs.at[m], hr.at[m], partner)

    def h_wait(m):
        h_all(m).wait_recv()

    def r_copy(b, m):
        return remote(
            obuf.at[b, m - 1], rbuf.at[b, group_rows(g)], es.at[b, m], rr.at[b, m], at_g(m)
        )

    def a_copy(b, side):
        return remote(obuf.at[b, far - 1], abuf.at[side], as_.at[side], ar.at[side], at_z(z + 1 - 2 * side))

    def rows_of(t):
        return pl.ds(pl.multiple_of(t * step, 16), step)

    def y_copy(b, side, t):
        to = z + 1 - 2 * side
        slot = jnp.where(jnp.logical_and(to == b, side == 1), L, b)
        return remote(zbuf.at[b, rows_of(t)], rin.at[slot, rows_of(t)], ys.at[b], yr.at[slot, t], at_z(to))

    def y_wait(slot, t):
        area = rin.at[slot, rows_of(t)]
        remote(area, area, ys.at[0], yr.at[slot, t], partner).wait_recv()

    def stat_copy(buf, send, recv, k):
        to = lax.rem(me + k, n)
        return remote(buf.at[me], buf.at[me], send.at[0], recv.at[0], {"tp": to})

    def stat_all(buf, send, recv):
        area = buf.at[0 : n - 1]
        return remote(area, area, send.at[0], recv.at[0], partner)

    barrier = pltpu.get_barrier_semaphore()
    for k in range(1, n):
        pl.semaphore_signal(barrier, inc=1, device_id={"tp": lax.rem(me + k, n)}, device_id_type=MESH)
    for m in range(1, G):
        pl.semaphore_signal(barrier, inc=1, device_id=at_g(m), device_id_type=MESH)
    x_load = pltpu.make_async_copy(x_ref, zbuf.at[z], xs.at[0])
    x_load.start()
    for s in range(2):
        for i in range(2):
            w_load(s, i).start()

    @pl.loop(0, L)
    def _(b):
        down_own(b).start()

    x_load.wait()
    stat[me, 0:nb] = squares_of(zbuf[z].astype(F32), nb)
    pre = pre_ref[...].astype(F32).reshape(1, cols)
    for c in range(cols // LANES):
        stat[me, nb + c : nb + c + 1] = pre[:, c * LANES : (c + 1) * LANES]

    pl.semaphore_wait(barrier, n + G - 2)
    for k in range(1, n):
        stat_copy(stat, ss, sr, k).start()
    pl.when(z < L - 1)(z_copy(z, 0).start)
    pl.when(z > 0)(z_copy(z, 1).start)

    ids, weights = ids_ref[...], rw_ref[...]
    top = ids.shape[0]
    id_rows = [fold(ids[t : t + 1], nb) for t in range(top)]
    weight_rows = [fold(weights[t : t + 1], nb) for t in range(top)]
    members, shares = [], []
    for e in range(G):
        named = [r == e for r in id_rows]
        members.append(sum(jnp.where(q, 1.0, 0.0) for q in named))
        shares.append(sum(jnp.where(q, w, 0.0) for q, w in zip(named, weight_rows)))
    member = jnp.concatenate(members, axis=0)
    small = member.astype(BF16)
    lane_a = lax.broadcasted_iota(jnp.int32, (LANES, LANES), 0)
    lane_b = lax.broadcasted_iota(jnp.int32, (LANES, LANES), 1)
    both = jnp.concatenate(
        [jnp.where(lane_a < lane_b, 1.0, 0.0).astype(BF16), jnp.ones((LANES, LANES), BF16)], axis=1
    )
    counted = jnp.dot(small, both, preferred_element_type=F32)
    row_a = lax.broadcasted_iota(jnp.int32, (G * nb, G * nb), 0)
    row_b = lax.broadcasted_iota(jnp.int32, (G * nb, G * nb), 1)
    ahead = jnp.where(jnp.logical_and(row_a // nb == row_b // nb, row_b < row_a), 1.0, 0.0).astype(BF16)
    rank = counted[:, :LANES] + jnp.dot(
        ahead, counted[:, LANES:].astype(BF16), preferred_element_type=F32
    )
    base = (lax.broadcasted_iota(jnp.int32, (G * nb, LANES), 0) // nb * cap).astype(F32)
    key = jnp.where(member > 0.5, rank + base, -1.0)
    kbuf[...] = key.astype(jnp.int32)
    kcol[...] = columns_of(key).astype(jnp.int32)
    wcol[...] = columns_of(jnp.concatenate(shares, axis=0))

    for e in range(G):
        wanted = lax.broadcasted_iota(jnp.int32, (cap, LANES), 0) + e * cap
        for r in range(nb):
            l, lane = r * LANES // cols, r * LANES % cols
            rbuf[l, e * cap : (e + 1) * cap, lane : lane + LANES] = jnp.where(
                kbuf[e * nb + r : e * nb + r + 1] == wanted, 1.0, 0.0
            ).astype(BF16)

    def row_scale(buf, send, recv):
        stat_all(buf, send, recv).wait_recv()
        total = buf[0, 0:nb]
        for k in range(1, n):
            total = total + buf[k, 0:nb]
        return columns_of(lax.rsqrt(total / width + epsilon))

    scol[...] = row_scale(stat, ss, sr)

    @pl.loop(0, L)
    def _(b):
        down_push(b).start()

    def take(s):
        b = order(s)
        z_copy(b, 0).wait_recv()
        pl.when(jnp.logical_and(b < z, z < L - 1))(z_copy(b, 0).start)
        pl.when(jnp.logical_and(b > z, z > 0))(z_copy(b, 1).start)

    def process(s):
        b = order(s)
        gain = jnp.concatenate(
            [stat[b * 2 + core, nb + c : nb + c + 1] for c in range(cols // LANES)], axis=1
        )
        for r in range(nb):
            at = slice(r * LANES, (r + 1) * LANES)
            nbuf[at] = (zbuf[b, at].astype(F32) * scol[:, r : r + 1] * gain).astype(BF16)

        @pl.loop(0, G)
        def _(j):
            m = G - 1 - j

            @pl.when(jnp.logical_not(jnp.logical_and(m == far, skipped(b))))
            def _():
                at = group_rows(flip(g, m, G))
                chooser = jnp.concatenate([rbuf[l, at] for l in range(tok // cols)], axis=1)
                chosen = jnp.dot(chooser, nbuf[...], preferred_element_type=F32).astype(BF16)

                @pl.when(m > 0)
                def _():
                    obuf[b, m - 1] = chosen
                    e_copy(b, m).start()

                @pl.when(m == 0)
                def _():
                    piece[core, b, group_rows(g)] = chosen
                    d_copy(b, 0).start()

    def gate_up(b, slot, at):
        left = jnp.concatenate([piece[0, b, at], piece[1, b, at]], axis=1)
        return [jnp.dot(left, wbuf[slot, i], preferred_element_type=F32) for i in range(2)]

    per = rows // tok
    blocks = rows // cols

    def mix_place(k):
        return k // per % 2, order(k // (2 * per)), (k % per) * tok

    def build_mix(q):
        b = order(q)

        d_sent(b)
        if q == 0:
            pl.when(z < L - 2)(f_copy(0).wait_send)
            pl.when(z > 1)(f_copy(1).wait_send)
        for k in range(2 * per * q, min(2 * per * (q + 1), blocks)):
            c, b, first = mix_place(k)
            lane = lax.broadcasted_iota(jnp.int32, (LANES, cols), 1) + k * cols
            for r in range(nb):
                value = jnp.zeros((LANES, cols), F32)
                for e in range(k * cols // cap, ((k + 1) * cols - 1) // cap + 1):
                    p = e * nb + r
                    value = jnp.where(kcol[:, p : p + 1] == lane, wcol[:, p : p + 1], value)
                piece[c, b, first + r * LANES : first + (r + 1) * LANES] = value.astype(BF16)

    def finish(s):
        b, slot = order(s), s % 2

        for q in range(L - 3):
            pl.when(s == q + 1)(functools.partial(build_mix, q))

        @pl.loop(1, G)
        def _(j):
            m = G - j
            e_copy(b, m).wait_recv()

            @pl.when(jnp.logical_and(m == far, b == z))
            def _():
                pl.when(z < L - 2)(f_copy(0).start)
                pl.when(z > 1)(f_copy(1).start)

            d_copy(b, m).start()

        @pl.loop(0, G)
        def _(m):
            d_copy(b, m).wait_recv()

        for i in range(2):
            w_load(s, i).wait()

        @pl.loop(0, rows // tile)
        def _(t):
            at = pl.ds(pl.multiple_of(t * tile, 16), tile)
            both = gate_up(b, slot, at)

            @pl.when(s == 0)
            def _():
                for i in range(2):
                    acc[i, at] = both[i]

            @pl.when(s > 0)
            def _():
                for i in range(2):
                    acc[i, at] += both[i]

        @pl.when(s + 2 < L)
        def _():
            for i in range(2):
                w_load(s + 2, i).start()

    @pl.loop(0, L)
    def _(s):
        early = jnp.logical_and(inside, s > 0)
        low = jnp.where(jnp.logical_and(early, s > 1), s + 1, s)
        high = jnp.where(early, jnp.minimum(s + 2, L), s + 1)

        @pl.when(s > 0)
        def _():
            pl.loop(low, high)(take)

        pl.loop(low, high)(process)

        @pl.when(jnp.logical_and(next_to_end, s == L - 1))
        def _():
            e_copy(farthest, far).wait_recv()
            l_copy().start()

        pl.when(jnp.logical_and(s > 0, s < L - 1))(lambda: finish(s - 1))

    def extra(b, side):
        if side == 0:
            return jnp.logical_and(z > 0, b == jnp.where(z > 1, z, L - 1))
        return jnp.logical_and(z < L - 1, b == jnp.where(z < L - 2, z, 0))

    def add_extra(b, held):
        for side in range(2):
            @pl.when(extra(b, side))
            def _():
                a_copy(b, side).wait_recv()
                held[0:cap] += abuf[side].astype(F32)

        obuf[b, far - 1] = held[0:cap].astype(BF16)

    def project(i, m):
        b = order(L - 1 - i)
        at = group_rows(flip(g, m, G))
        if units % LANES == 0:
            left = jnp.concatenate([hbuf[0, at], hbuf[1, at]], axis=1)
            result = jnp.dot(left, dbuf[b], preferred_element_type=F32)
        else:
            result = jnp.dot(hbuf[0, at], dbuf[b, 0:units], preferred_element_type=F32)
            result += jnp.dot(hbuf[1, at], dbuf[b, units:], preferred_element_type=F32)

        @pl.when(m == 0)
        def _():
            rbuf[b, at] = result.astype(BF16)

        @pl.when(jnp.logical_and(m > 0, m < far))
        def _():
            e_copy(b, m).wait_send()
            obuf[b, m - 1] = result.astype(BF16)

        @pl.when(m == far)
        def _():
            @pl.when(skipped(b))
            def _():
                obuf[b, far - 1] = result.astype(BF16)
                to_right = jnp.where(inside, b > z, z == 0)
                pl.when(to_right)(a_copy(b, 0).start)
                pl.when(jnp.logical_not(to_right))(a_copy(b, 1).start)

            @pl.when(jnp.logical_not(skipped(b)))
            def _():
                e_copy(b, far).wait_send()

                @pl.when(i > 0)
                def _():
                    tbuf[0:cap] = result

                @pl.when(i == 0)
                def _():
                    ebuf[...] = result

    def sent(b, m):
        return jnp.logical_not(jnp.logical_and(m == far, skipped(b)))

    def wait_sends(i):
        b = order(L - 1 - i)

        @pl.loop(1, G)
        def _(m):
            pl.when(sent(b, m))(lambda: r_copy(b, m).wait_send())

    def start_sends(b):
        @pl.loop(0, far)
        def _(j):
            m = far - j
            pl.when(sent(b, m))(lambda: r_copy(b, m).start())

    def down_ready():
        down_all(dps, dl).wait_recv()
        down_all(dps, dpr).wait_recv()

    before = second = order(L - 2)

    def take_before(m):
        d_copy(before, m).wait_recv()
        at = group_rows(flip(g, m, G))
        both = gate_up(before, (L - 2) % 2, at)
        for i in range(2):
            acc[i, at] += both[i]

    def close(m):
        d_copy(last, m).wait_recv()

        @pl.loop(0, cap // half)
        def _(t):
            at = pl.ds(pl.multiple_of(flip(g, m, G) * cap + t * half, 16), half)
            both = gate_up(last, (L - 1) % 2, at)
            gates = 0.5 * (both[0] + acc[0, at])
            hbuf[core, at] = ((gates + gates * jnp.tanh(gates)) * (both[1] + acc[1, at])).astype(BF16)
            h_copy(m, t).start()

    build_mix(L - 3)

    @pl.loop(1, G)
    def _(m):
        e_copy(before, m).wait_recv()
        d_copy(before, m).start()

    for s in (L - 2, L - 1):
        for i in range(2):
            w_load(s, i).wait()
    down_ready()

    @pl.loop(0, 2 * far + 1)
    def _(v):
        u = v - far
        pl.when(jnp.logical_or(v < far, u == far))(lambda: take_before(jnp.minimum(v, far)))

        @pl.when(v == 1)
        def _():
            @pl.loop(1, far)
            def _(k):
                e_copy(last, k).wait_recv()
                d_copy(last, k).start()

        @pl.when(u == far - 1)
        def _():
            @pl.when(jnp.logical_not(next_to_end))
            def _():
                e_copy(last, far).wait_recv()

            d_copy(last, far).start()

        @pl.when(jnp.logical_or(v == 0, jnp.logical_and(u >= 0, u != far - 1)))
        def _():
            close(jnp.where(v == 0, 0, jnp.minimum(u + 1, far)))

        @pl.when(jnp.logical_and(u > 0, u < far))
        def _():
            h_wait(u)
            project(0, u)
            r_copy(last, u).start()

    def first_far():
        obuf[last, far - 1] = ebuf[...].astype(BF16)
        r_copy(last, far).start()

    def after_dispatch():
        build_mix(L - 2)
        pl.when(z < L - 1)(z_copy(z, 0).wait_send)
        pl.when(z > 0)(z_copy(z, 1).wait_send)
        pl.when(next_to_end)(l_copy().wait_send)

        @pl.loop(0, L)
        def _(b):
            pl.when(jnp.logical_and(b < z, z < L - 1))(z_copy(b, 0).wait_send)
            pl.when(jnp.logical_and(b > z, z > 0))(z_copy(b, 1).wait_send)

            @pl.when(skipped(b))
            def _():
                rbuf[b, group_rows(flip(g, far, G))] = jnp.zeros((cap, cols), BF16)

    def combined(b, t):
        parts = []
        for k in range(blocks):
            c, l, first = mix_place(k)
            parts.append(piece[c, l, pl.ds(pl.multiple_of(first + t * step, 16), step)])
        return jnp.dot(jnp.concatenate(parts, axis=1), rbuf[b], preferred_element_type=F32)

    def arrived(b):
        @pl.loop(1, G)
        def _(m):
            @pl.when(jnp.logical_not(jnp.logical_and(m == far, skipped(b))))
            def _():
                r_copy(b, m).wait_recv()

    def combine(i):
        b = order(L - 1 - i)
        own = b == z
        more = jnp.logical_and(jnp.logical_not(own), jnp.where(b > z, z, L - 1 - z) > 0)
        ends_here = jnp.logical_or(own, more)
        arrived(b)

        @pl.loop(0, tiles)
        def _(t):
            at = rows_of(t)
            value = combined(b, t)

            @pl.when(own)
            def _():
                tbuf[at] = value

            @pl.when(more)
            def _():
                y_wait(b, t)
                zbuf[b, at] = (value + rin[b, at].astype(F32)).astype(BF16)

            @pl.when(jnp.logical_not(ends_here))
            def _():
                zbuf[b, at] = value.astype(BF16)

            pl.when(b > z)(y_copy(b, 0, t).start)
            pl.when(b < z)(y_copy(b, 1, t).start)

    def launch(i):
        b = order(L - 1 - i)

        @pl.when(jnp.logical_and(next_to_end, i == 2))
        def _():
            add_extra(last, ebuf)
            r_copy(last, far).start()

        pl.when(sent(b, far))(lambda: add_extra(b, tbuf))
        pl.when(jnp.logical_or(i > 1, jnp.logical_not(inside)))(lambda: wait_sends(i - 1))
        start_sends(b)

    late = jnp.where(inside, 2, 1)

    @pl.loop(1, L + 2)
    def _(i):
        first = i == 1

        @pl.when(i < L)
        def _():
            @pl.loop(0, jnp.where(first, G + 2, G))
            def _(j):
                pl.when(jnp.logical_and(first, j == far - 1))(lambda: h_wait(far))
                pl.when(jnp.logical_and(first, j == far + 1))(lambda: h_wait(0))
                m = jnp.where(first, jnp.where(j < far, j + 1, jnp.where(j == far, far, 0)), far - j)
                rest = jnp.logical_and(first, jnp.logical_or(j == far, j == far + 1))
                project(jnp.where(rest, 0, i), m)
                pl.when(j == far - 1)(lambda: launch(i))

        @pl.when(first)
        def _():
            pl.when(jnp.logical_not(jnp.logical_or(skipped(last), next_to_end)))(first_far)
            after_dispatch()

        c = i - late
        pl.when(jnp.logical_and(c >= 0, c < L))(lambda: combine(c))

    @pl.loop(0, tiles)
    def _(t):
        at = rows_of(t)
        for side, slot in ((0, z), (1, L)):
            @pl.when(z > 0 if side == 0 else z < L - 1)
            def _():
                y_wait(slot, t)
                tbuf[at] += rin[slot, at].astype(F32)

    def out_copy(t):
        at = slice(t * LANES, (t + 1) * LANES)
        return pltpu.make_async_copy(nbuf.at[at], out_ref.at[at], xs.at[0])

    stat2[me] = squares_of(tbuf[...], nb)
    for k in range(1, n):
        stat_copy(stat2, ts, tr, k).start()
    stat_all(stat, ss, sr).wait_send()

    pl.when(z == 0)(a_copy(farthest, 0).wait_send)
    pl.when(z == L - 1)(a_copy(farthest, 1).wait_send)

    @pl.when(inside)
    def _():
        a_copy(z + 1, 0).wait_send()
        a_copy(z - 1, 1).wait_send()

    pl.when(inside)(lambda: wait_sends(0))
    wait_sends(L - 1)

    down_all(dps, dpr).wait_send()

    @pl.loop(0, L)
    def _(b):
        @pl.when(b != z)
        def _():
            remote(zbuf.at[b], zbuf.at[b], ys.at[b], zr.at[b], partner).wait_send()

    d_sent(last)

    @pl.loop(0, G)
    def _(m):
        h_all(m).wait_send()

    tbuf[...] = tbuf[...] * post_ref[...].astype(F32).reshape(1, cols)
    scale = row_scale(stat2, ts, tr)
    for r in range(nb):
        at = slice(r * LANES, (r + 1) * LANES)
        nbuf[at] = (tbuf[at] * scale[:, r : r + 1]).astype(BF16)
        out_copy(r).start()

    stat_all(stat2, ts, tr).wait_send()
    pltpu.make_async_copy(nbuf, out_ref, xs.at[0]).wait()


def on_device(
    tokens, pre_gain, route_ids, route_weights, gate_weight, up_weight, down_weight, post_gain
):
    tok, cols = tokens.shape
    top = route_ids.shape[1]
    G = lax.axis_size("ep")
    n = lax.axis_size("tp")
    L = n // 2
    cap = 9 * tok * top // (8 * G)
    rows = G * cap
    units = gate_weight.shape[2]
    nb = tok // LANES
    tile = cap
    tiles = tok // min(256, tok)
    vmem = pl.BlockSpec(memory_space=pltpu.VMEM)
    hbm = pl.BlockSpec(memory_space=pl.ANY)
    return pl.pallas_call(
        functools.partial(layer_kernel, L, G, cap, tile),
        out_shape=jax.ShapeDtypeStruct((tok, cols), BF16),
        in_specs=[hbm] + [vmem] * 4 + [hbm] * 3,
        out_specs=hbm,
        scratch_shapes=[
            pltpu.VMEM((L, tok, cols), BF16),
            pltpu.VMEM((tok, cols), BF16),
            pltpu.VMEM((L, G - 1, cap, cols), BF16),
            pltpu.VMEM((2, L, rows, cols), BF16),
            pltpu.VMEM((2, 2, 2 * cols, units), BF16),
            pltpu.VMEM((2, rows, units), F32),
            pltpu.VMEM((2, rows, units), BF16),
            pltpu.VMEM((L, 2 * units, cols), BF16),
            pltpu.VMEM((L, rows, cols), BF16),
            pltpu.VMEM((L + 1, tok, cols), BF16),
            pltpu.VMEM((2, cap, cols), BF16),
            pltpu.VMEM((cap, cols), F32),
            pltpu.VMEM((tok, cols), F32),
            pltpu.VMEM((n, 2 * nb, LANES), F32),
            pltpu.VMEM((n, nb, LANES), F32),
            pltpu.VMEM((G * nb, LANES), jnp.int32),
            pltpu.VMEM((LANES, LANES), jnp.int32),
            pltpu.VMEM((LANES, LANES), F32),
            pltpu.VMEM((LANES, LANES), F32),
            DMA((2, L)), DMA((L,)),
            DMA((L, G)), DMA((L, G)),
            DMA((3,)),
            DMA((L,)), DMA((L, G)),
            DMA((2, 2)),
            DMA((1,)), DMA((1,)), DMA((1,)),
            DMA((G,)), DMA((G,)),
            DMA((L, G)),
            DMA((2,)), DMA((2,)),
            DMA((L,)), DMA((L + 1, tiles)),
            DMA((1,)), DMA((1,)),
            DMA((1,)), DMA((1,)),
            DMA((1,)),
        ],
        compiler_params=pltpu.CompilerParams(
            collective_id=1, has_side_effects=True, vmem_limit_bytes=62 * 2**20
        ),
        name="layer",
    )(
        tokens, pre_gain, post_gain, route_ids.T, route_weights.T,
        gate_weight[0], up_weight[0], down_weight[0],
    )


def solution(mesh):
    placed = (
        P("ep", "tp"),
        P("tp"),
        P("ep", None),
        P("ep", None),
        P("ep", None, "tp"),
        P("ep", None, "tp"),
        P("ep", "tp", None),
        P("tp"),
    )
    return jax.shard_map(
        on_device, mesh=mesh, in_specs=placed, out_specs=P("ep", "tp"), check_vma=False
    )
```

```python
import functools

import jax
import jax.numpy as jnp
from jax import lax
from jax.experimental import pallas as pl
from jax.experimental.pallas import tpu as pltpu
from jax.sharding import PartitionSpec as P

epsilon = 1e-06
MESH = pl.DeviceIdType.MESH
DMA = pltpu.SemaphoreType.DMA
BF16 = jnp.bfloat16
F32 = jnp.float32
LANES = 128


def flip(a, m, size):
    total, bit = 0, 1
    while bit < size:
        total = total + (((a // bit) % 2 + (m // bit) % 2) % 2) * bit
        bit *= 2
    return total


def columns_of(values):
    rows = values.shape[0]
    if rows < LANES:
        values = jnp.concatenate([values, jnp.zeros((LANES - rows, LANES), values.dtype)], axis=0)
    return values.T


def fold(wide, nb):
    row = lax.broadcasted_iota(jnp.int32, (nb, LANES), 0)
    total = None
    for r in range(nb):
        part = jnp.broadcast_to(wide[:, r * LANES : (r + 1) * LANES], (nb, LANES))
        total = part if total is None else jnp.where(row == r, part, total)
    return total


def squares_of(v, nb):
    square = v * v
    high = square.astype(BF16)
    low = (square - high.astype(F32)).astype(BF16)
    ones = jnp.ones((nb, v.shape[1]), BF16)
    dims = (((1,), (1,)), ((), ()))
    wide = lax.dot_general(ones, high, dims, preferred_element_type=F32)
    wide += lax.dot_general(ones, low, dims, preferred_element_type=F32)
    return fold(wide, nb)


def layer_kernel(
    L, G, cap, tile,
    x_ref, pre_ref, post_ref, ids_ref, rw_ref, gate_ref, up_ref, down_ref, out_ref,
    zbuf, nbuf, obuf, piece, wbuf, acc, hbuf, dbuf, rbuf, rin, abuf, ebuf, tbuf,
    stat, stat2, kbuf, kcol, wcol, scol,
    zs, zr, es, er, fs, ds, dr, ws, dl, dps, dpr, hs, hr, rr, as_, ar, ys, yr, ss, sr, ts, tr, xs,
):
    tok, cols = nbuf.shape
    nb = tok // LANES
    n = 2 * L
    units = gate_ref.shape[1]
    rows = G * cap
    far = G - 1
    me, g = lax.axis_index("tp"), lax.axis_index("ep")
    core, z = lax.rem(me, 2), me // 2
    partner = {"tp": me + 1 - 2 * core}
    inside = jnp.logical_and(z > 0, z < L - 1)
    inner = jnp.minimum(z, L - 1 - z)
    width = n * cols
    step = min(256, tok)
    tiles = tok // step

    def order(s):
        near = jnp.where(s % 2 == 1, z - (s + 1) // 2, z + (s + 1) // 2)
        rest = jnp.where(2 * z > L - 1, z - (s - inner), z + (s - inner))
        return jnp.where(s <= 2 * inner, near, rest)

    farthest = jnp.where(2 * z > L - 1, 0, L - 1)
    last = order(L - 1)
    end_left = z == 1
    next_to_end = jnp.logical_or(z == 1, z == L - 2)

    def skipped(b):
        beside = jnp.logical_or(b == z + 1, b == z - 1)
        return jnp.where(inside, beside, b == farthest)

    def group_rows(e):
        return pl.ds(pl.multiple_of(e * cap, 16), cap)

    def remote(src, dst, send, recv, to):
        return pltpu.make_async_remote_copy(
            src_ref=src, dst_ref=dst, send_sem=send, recv_sem=recv, device_id=to, device_id_type=MESH
        )

    def at_z(to):
        return {"tp": to * 2 + core}

    def at_g(m):
        return {"ep": flip(g, m, G)}

    def w_load(s, i):
        ref = (gate_ref, up_ref)[i]
        depth = pl.ds(pl.multiple_of(order(s) * 2 * cols, LANES), 2 * cols)
        return pltpu.make_async_copy(ref.at[depth], wbuf.at[s % 2, i], ws.at[s % 2, i])

    def my_units(c):
        return pl.ds(pl.multiple_of(c * units, 16), units)

    def down_part(b, c):
        return down_ref.at[:, pl.ds(pl.multiple_of((b * 2 + c) * cols, LANES), cols)]

    def down_own(b):
        return pltpu.make_async_copy(down_part(b, core), dbuf.at[b, my_units(core)], dl.at[0])

    def down_push(b):
        return remote(
            down_part(b, 1 - core), dbuf.at[b, my_units(core)], dps.at[0], dpr.at[0], partner
        )

    def down_all(send, recv):
        area = dbuf.at[:, my_units(core)]
        return remote(area, area, send.at[0], recv.at[0], partner)

    def z_copy(b, side):
        return remote(zbuf.at[b], zbuf.at[b], zs.at[side, b], zr.at[b], at_z(z + 1 - 2 * side))

    def e_copy(b, m):
        return remote(
            obuf.at[b, m - 1], piece.at[core, b, group_rows(g)], es.at[b, m], er.at[b, m], at_g(m)
        )

    def f_copy(side):
        area = piece.at[core, z, group_rows(flip(g, far, G))]
        return remote(area, area, fs.at[side], er.at[z, far], at_z(z + 1 - 2 * side))

    def l_copy():
        area = piece.at[core, farthest, group_rows(flip(g, far, G))]
        return remote(area, area, fs.at[2], er.at[farthest, far], at_z(jnp.where(end_left, 0, L - 1)))

    def d_copy(b, m):
        area = piece.at[core, b, group_rows(flip(g, m, G))]
        return remote(area, area, ds.at[b], dr.at[b, m], partner)

    half = cap // 2 if cap % 32 == 0 else cap

    def d_sent(b):
        area = piece.at[core, b]
        remote(area, area, ds.at[b], dr.at[b, 0], partner).wait_send()

    def h_copy(m, t):
        at = pl.ds(pl.multiple_of(flip(g, m, G) * cap + t * half, 16), half)
        area = hbuf.at[core, at]
        return remote(area, area, hs.at[m], hr.at[m], partner)

    def h_all(m):
        area = hbuf.at[core, group_rows(flip(g, m, G))]
        return remote(area, area, hs.at[m], hr.at[m], partner)

    def h_wait(m):
        h_all(m).wait_recv()

    def r_copy(b, m):
        return remote(
            obuf.at[b, m - 1], rbuf.at[b, group_rows(g)], es.at[b, m], rr.at[b, m], at_g(m)
        )

    def a_copy(b, side):
        return remote(obuf.at[b, far - 1], abuf.at[side], as_.at[side], ar.at[side], at_z(z + 1 - 2 * side))

    def rows_of(t):
        return pl.ds(pl.multiple_of(t * step, 16), step)

    def y_copy(b, side, t):
        to = z + 1 - 2 * side
        slot = jnp.where(jnp.logical_and(to == b, side == 1), L, b)
        return remote(zbuf.at[b, rows_of(t)], rin.at[slot, rows_of(t)], ys.at[b], yr.at[slot, t], at_z(to))

    def y_wait(slot, t):
        area = rin.at[slot, rows_of(t)]
        remote(area, area, ys.at[0], yr.at[slot, t], partner).wait_recv()

    def stat_copy(buf, send, recv, k):
        to = lax.rem(me + k, n)
        return remote(buf.at[me], buf.at[me], send.at[0], recv.at[0], {"tp": to})

    def stat_all(buf, send, recv):
        area = buf.at[0 : n - 1]
        return remote(area, area, send.at[0], recv.at[0], partner)

    barrier = pltpu.get_barrier_semaphore()
    for k in range(1, n):
        pl.semaphore_signal(barrier, inc=1, device_id={"tp": lax.rem(me + k, n)}, device_id_type=MESH)
    for m in range(1, G):
        pl.semaphore_signal(barrier, inc=1, device_id=at_g(m), device_id_type=MESH)
    x_load = pltpu.make_async_copy(x_ref, zbuf.at[z], xs.at[0])
    x_load.start()
    for s in range(2):
        for i in range(2):
            w_load(s, i).start()

    @pl.loop(0, L)
    def _(b):
        down_own(b).start()

    x_load.wait()
    stat[me, 0:nb] = squares_of(zbuf[z].astype(F32), nb)
    pre = pre_ref[...].astype(F32).reshape(1, cols)
    for c in range(cols // LANES):
        stat[me, nb + c : nb + c + 1] = pre[:, c * LANES : (c + 1) * LANES]

    pl.semaphore_wait(barrier, n + G - 2)
    for k in range(1, n):
        stat_copy(stat, ss, sr, k).start()
    pl.when(z < L - 1)(z_copy(z, 0).start)
    pl.when(z > 0)(z_copy(z, 1).start)

    ids, weights = ids_ref[...], rw_ref[...]
    top = ids.shape[0]
    id_rows = [fold(ids[t : t + 1], nb) for t in range(top)]
    weight_rows = [fold(weights[t : t + 1], nb) for t in range(top)]
    members, shares = [], []
    for e in range(G):
        named = [r == e for r in id_rows]
        members.append(sum(jnp.where(q, 1.0, 0.0) for q in named))
        shares.append(sum(jnp.where(q, w, 0.0) for q, w in zip(named, weight_rows)))
    member = jnp.concatenate(members, axis=0)
    small = member.astype(BF16)
    lane_a = lax.broadcasted_iota(jnp.int32, (LANES, LANES), 0)
    lane_b = lax.broadcasted_iota(jnp.int32, (LANES, LANES), 1)
    both = jnp.concatenate(
        [jnp.where(lane_a < lane_b, 1.0, 0.0).astype(BF16), jnp.ones((LANES, LANES), BF16)], axis=1
    )
    counted = jnp.dot(small, both, preferred_element_type=F32)
    row_a = lax.broadcasted_iota(jnp.int32, (G * nb, G * nb), 0)
    row_b = lax.broadcasted_iota(jnp.int32, (G * nb, G * nb), 1)
    ahead = jnp.where(jnp.logical_and(row_a // nb == row_b // nb, row_b < row_a), 1.0, 0.0).astype(BF16)
    rank = counted[:, :LANES] + jnp.dot(
        ahead, counted[:, LANES:].astype(BF16), preferred_element_type=F32
    )
    base = (lax.broadcasted_iota(jnp.int32, (G * nb, LANES), 0) // nb * cap).astype(F32)
    key = jnp.where(member > 0.5, rank + base, -1.0)
    kbuf[...] = key.astype(jnp.int32)
    kcol[...] = columns_of(key).astype(jnp.int32)
    wcol[...] = columns_of(jnp.concatenate(shares, axis=0))

    for e in range(G):
        wanted = lax.broadcasted_iota(jnp.int32, (cap, LANES), 0) + e * cap
        for r in range(nb):
            l, lane = r * LANES // cols, r * LANES % cols
            rbuf[l, e * cap : (e + 1) * cap, lane : lane + LANES] = jnp.where(
                kbuf[e * nb + r : e * nb + r + 1] == wanted, 1.0, 0.0
            ).astype(BF16)

    def row_scale(buf, send, recv):
        stat_all(buf, send, recv).wait_recv()
        total = buf[0, 0:nb]
        for k in range(1, n):
            total = total + buf[k, 0:nb]
        return columns_of(lax.rsqrt(total / width + epsilon))

    scol[...] = row_scale(stat, ss, sr)

    @pl.loop(0, L)
    def _(b):
        down_push(b).start()

    def take(s):
        b = order(s)
        z_copy(b, 0).wait_recv()
        pl.when(jnp.logical_and(b < z, z < L - 1))(z_copy(b, 0).start)
        pl.when(jnp.logical_and(b > z, z > 0))(z_copy(b, 1).start)

    def process(s):
        b = order(s)
        gain = jnp.concatenate(
            [stat[b * 2 + core, nb + c : nb + c + 1] for c in range(cols // LANES)], axis=1
        )
        for r in range(nb):
            at = slice(r * LANES, (r + 1) * LANES)
            nbuf[at] = (zbuf[b, at].astype(F32) * scol[:, r : r + 1] * gain).astype(BF16)

        @pl.loop(0, G)
        def _(j):
            m = G - 1 - j

            @pl.when(jnp.logical_not(jnp.logical_and(m == far, skipped(b))))
            def _():
                at = group_rows(flip(g, m, G))
                chooser = jnp.concatenate([rbuf[l, at] for l in range(tok // cols)], axis=1)
                chosen = jnp.dot(chooser, nbuf[...], preferred_element_type=F32).astype(BF16)

                @pl.when(m > 0)
                def _():
                    obuf[b, m - 1] = chosen
                    e_copy(b, m).start()

                @pl.when(m == 0)
                def _():
                    piece[core, b, group_rows(g)] = chosen
                    d_copy(b, 0).start()

    def gate_up(b, slot, at):
        left = jnp.concatenate([piece[0, b, at], piece[1, b, at]], axis=1)
        return [jnp.dot(left, wbuf[slot, i], preferred_element_type=F32) for i in range(2)]

    per = rows // tok
    blocks = rows // cols

    def mix_place(k):
        return k // per % 2, order(k // (2 * per)), (k % per) * tok

    def build_mix(q):
        b = order(q)

        d_sent(b)
        if q == 0:
            pl.when(z < L - 2)(f_copy(0).wait_send)
            pl.when(z > 1)(f_copy(1).wait_send)
        for k in range(2 * per * q, min(2 * per * (q + 1), blocks)):
            c, b, first = mix_place(k)
            lane = lax.broadcasted_iota(jnp.int32, (LANES, cols), 1) + k * cols
            for r in range(nb):
                value = jnp.zeros((LANES, cols), F32)
                for e in range(k * cols // cap, ((k + 1) * cols - 1) // cap + 1):
                    p = e * nb + r
                    value = jnp.where(kcol[:, p : p + 1] == lane, wcol[:, p : p + 1], value)
                piece[c, b, first + r * LANES : first + (r + 1) * LANES] = value.astype(BF16)

    def finish(s):
        b, slot = order(s), s % 2

        for q in range(L - 3):
            pl.when(s == q + 1)(functools.partial(build_mix, q))

        @pl.loop(1, G)
        def _(j):
            m = G - j
            e_copy(b, m).wait_recv()

            @pl.when(jnp.logical_and(m == far, b == z))
            def _():
                pl.when(z < L - 2)(f_copy(0).start)
                pl.when(z > 1)(f_copy(1).start)

            d_copy(b, m).start()

        @pl.loop(0, G)
        def _(m):
            d_copy(b, m).wait_recv()

        for i in range(2):
            w_load(s, i).wait()

        @pl.loop(0, rows // tile)
        def _(t):
            at = pl.ds(pl.multiple_of(t * tile, 16), tile)
            both = gate_up(b, slot, at)

            @pl.when(s == 0)
            def _():
                for i in range(2):
                    acc[i, at] = both[i]

            @pl.when(s > 0)
            def _():
                for i in range(2):
                    acc[i, at] += both[i]

        @pl.when(s + 2 < L)
        def _():
            for i in range(2):
                w_load(s + 2, i).start()

    @pl.loop(0, L)
    def _(s):
        early = jnp.logical_and(inside, s > 0)
        low = jnp.where(jnp.logical_and(early, s > 1), s + 1, s)
        high = jnp.where(early, jnp.minimum(s + 2, L), s + 1)

        @pl.when(s > 0)
        def _():
            pl.loop(low, high)(take)

        pl.loop(low, high)(process)

        @pl.when(jnp.logical_and(next_to_end, s == L - 1))
        def _():
            e_copy(farthest, far).wait_recv()
            l_copy().start()

        pl.when(jnp.logical_and(s > 0, s < L - 1))(lambda: finish(s - 1))

    def extra(b, side):
        if side == 0:
            return jnp.logical_and(z > 0, b == jnp.where(z > 1, z, L - 1))
        return jnp.logical_and(z < L - 1, b == jnp.where(z < L - 2, z, 0))

    def add_extra(b, held):
        for side in range(2):
            @pl.when(extra(b, side))
            def _():
                a_copy(b, side).wait_recv()
                held[0:cap] += abuf[side].astype(F32)

        obuf[b, far - 1] = held[0:cap].astype(BF16)

    def project(i, m):
        b = order(L - 1 - i)
        at = group_rows(flip(g, m, G))
        if units % LANES == 0:
            left = jnp.concatenate([hbuf[0, at], hbuf[1, at]], axis=1)
            result = jnp.dot(left, dbuf[b], preferred_element_type=F32)
        else:
            result = jnp.dot(hbuf[0, at], dbuf[b, 0:units], preferred_element_type=F32)
            result += jnp.dot(hbuf[1, at], dbuf[b, units:], preferred_element_type=F32)

        @pl.when(m == 0)
        def _():
            rbuf[b, at] = result.astype(BF16)

        @pl.when(jnp.logical_and(m > 0, m < far))
        def _():
            e_copy(b, m).wait_send()
            obuf[b, m - 1] = result.astype(BF16)

        @pl.when(m == far)
        def _():
            @pl.when(skipped(b))
            def _():
                obuf[b, far - 1] = result.astype(BF16)
                to_right = jnp.where(inside, b > z, z == 0)
                pl.when(to_right)(a_copy(b, 0).start)
                pl.when(jnp.logical_not(to_right))(a_copy(b, 1).start)

            @pl.when(jnp.logical_not(skipped(b)))
            def _():
                e_copy(b, far).wait_send()

                @pl.when(i > 0)
                def _():
                    tbuf[0:cap] = result

                @pl.when(i == 0)
                def _():
                    ebuf[...] = result

    def sent(b, m):
        return jnp.logical_not(jnp.logical_and(m == far, skipped(b)))

    def wait_sends(i):
        b = order(L - 1 - i)

        @pl.loop(1, G)
        def _(m):
            pl.when(sent(b, m))(lambda: r_copy(b, m).wait_send())

    def start_sends(b):
        @pl.loop(0, far)
        def _(j):
            m = far - j
            pl.when(sent(b, m))(lambda: r_copy(b, m).start())

    def down_ready():
        down_all(dps, dl).wait_recv()
        down_all(dps, dpr).wait_recv()

    before = second = order(L - 2)

    def take_before(m):
        d_copy(before, m).wait_recv()
        at = group_rows(flip(g, m, G))
        both = gate_up(before, (L - 2) % 2, at)
        for i in range(2):
            acc[i, at] += both[i]

    def close(m):
        d_copy(last, m).wait_recv()

        @pl.loop(0, cap // half)
        def _(t):
            at = pl.ds(pl.multiple_of(flip(g, m, G) * cap + t * half, 16), half)
            both = gate_up(last, (L - 1) % 2, at)
            gates = 0.5 * (both[0] + acc[0, at])
            hbuf[core, at] = ((gates + gates * jnp.tanh(gates)) * (both[1] + acc[1, at])).astype(BF16)
            h_copy(m, t).start()

    build_mix(L - 3)

    @pl.loop(1, G)
    def _(m):
        e_copy(before, m).wait_recv()
        d_copy(before, m).start()

    for s in (L - 2, L - 1):
        for i in range(2):
            w_load(s, i).wait()
    down_ready()

    @pl.loop(0, 2 * far + 1)
    def _(v):
        u = v - far
        pl.when(v <= far)(lambda: take_before(v))

        @pl.when(v == far - 1)
        def _():
            @pl.loop(1, far)
            def _(k):
                e_copy(last, k).wait_recv()
                d_copy(last, k).start()

        @pl.when(u == far - 1)
        def _():
            @pl.when(jnp.logical_not(next_to_end))
            def _():
                e_copy(last, far).wait_recv()

            d_copy(last, far).start()

        @pl.when(jnp.logical_or(v == 0, jnp.logical_and(u >= 0, u != far - 1)))
        def _():
            close(jnp.where(v == 0, 0, jnp.minimum(u + 1, far)))

        @pl.when(jnp.logical_and(u > 0, u < far))
        def _():
            h_wait(u)
            project(0, u)
            r_copy(last, u).start()

    def first_far():
        obuf[last, far - 1] = ebuf[...].astype(BF16)
        r_copy(last, far).start()

    def after_dispatch():
        build_mix(L - 2)
        pl.when(z < L - 1)(z_copy(z, 0).wait_send)
        pl.when(z > 0)(z_copy(z, 1).wait_send)
        pl.when(next_to_end)(l_copy().wait_send)

        @pl.loop(0, L)
        def _(b):
            pl.when(jnp.logical_and(b < z, z < L - 1))(z_copy(b, 0).wait_send)
            pl.when(jnp.logical_and(b > z, z > 0))(z_copy(b, 1).wait_send)

            @pl.when(skipped(b))
            def _():
                rbuf[b, group_rows(flip(g, far, G))] = jnp.zeros((cap, cols), BF16)

    def combined(b, t):
        parts = []
        for k in range(blocks):
            c, l, first = mix_place(k)
            parts.append(piece[c, l, pl.ds(pl.multiple_of(first + t * step, 16), step)])
        return jnp.dot(jnp.concatenate(parts, axis=1), rbuf[b], preferred_element_type=F32)

    def arrived(b):
        @pl.loop(1, G)
        def _(m):
            @pl.when(jnp.logical_not(jnp.logical_and(m == far, skipped(b))))
            def _():
                r_copy(b, m).wait_recv()

    def combine(i):
        b = order(L - 1 - i)
        own = b == z
        more = jnp.logical_and(jnp.logical_not(own), jnp.where(b > z, z, L - 1 - z) > 0)
        ends_here = jnp.logical_or(own, more)
        arrived(b)

        @pl.loop(0, tiles)
        def _(t):
            at = rows_of(t)
            value = combined(b, t)

            @pl.when(own)
            def _():
                tbuf[at] = value

            @pl.when(more)
            def _():
                y_wait(b, t)
                zbuf[b, at] = (value + rin[b, at].astype(F32)).astype(BF16)

            @pl.when(jnp.logical_not(ends_here))
            def _():
                zbuf[b, at] = value.astype(BF16)

            pl.when(b > z)(y_copy(b, 0, t).start)
            pl.when(b < z)(y_copy(b, 1, t).start)

    def launch(i):
        b = order(L - 1 - i)

        @pl.when(jnp.logical_and(next_to_end, i == 2))
        def _():
            add_extra(last, ebuf)
            r_copy(last, far).start()

        pl.when(sent(b, far))(lambda: add_extra(b, tbuf))
        pl.when(jnp.logical_or(i > 1, jnp.logical_not(inside)))(lambda: wait_sends(i - 1))
        start_sends(b)

    late = jnp.where(inside, 2, 1)

    @pl.loop(1, L + 2)
    def _(i):
        first = i == 1

        @pl.when(i < L)
        def _():
            @pl.loop(0, jnp.where(first, G + 2, G))
            def _(j):
                pl.when(jnp.logical_and(first, j == far - 1))(lambda: h_wait(far))
                pl.when(jnp.logical_and(first, j == far + 1))(lambda: h_wait(0))
                m = jnp.where(first, jnp.where(j < far, j + 1, jnp.where(j == far, far, 0)), far - j)
                rest = jnp.logical_and(first, jnp.logical_or(j == far, j == far + 1))
                project(jnp.where(rest, 0, i), m)
                pl.when(j == far - 1)(lambda: launch(i))

        @pl.when(first)
        def _():
            pl.when(jnp.logical_not(jnp.logical_or(skipped(last), next_to_end)))(first_far)
            after_dispatch()

        c = i - late
        pl.when(jnp.logical_and(c >= 0, c < L))(lambda: combine(c))

    @pl.loop(0, tiles)
    def _(t):
        at = rows_of(t)
        for side, slot in ((0, z), (1, L)):
            @pl.when(z > 0 if side == 0 else z < L - 1)
            def _():
                y_wait(slot, t)
                tbuf[at] += rin[slot, at].astype(F32)

    def out_copy(t):
        at = slice(t * LANES, (t + 1) * LANES)
        return pltpu.make_async_copy(nbuf.at[at], out_ref.at[at], xs.at[0])

    stat2[me] = squares_of(tbuf[...], nb)
    for k in range(1, n):
        stat_copy(stat2, ts, tr, k).start()
    stat_all(stat, ss, sr).wait_send()

    pl.when(z == 0)(a_copy(farthest, 0).wait_send)
    pl.when(z == L - 1)(a_copy(farthest, 1).wait_send)

    @pl.when(inside)
    def _():
        a_copy(z + 1, 0).wait_send()
        a_copy(z - 1, 1).wait_send()

    pl.when(inside)(lambda: wait_sends(0))
    wait_sends(L - 1)

    down_all(dps, dpr).wait_send()

    @pl.loop(0, L)
    def _(b):
        @pl.when(b != z)
        def _():
            remote(zbuf.at[b], zbuf.at[b], ys.at[b], zr.at[b], partner).wait_send()

    d_sent(last)

    @pl.loop(0, G)
    def _(m):
        h_all(m).wait_send()

    tbuf[...] = tbuf[...] * post_ref[...].astype(F32).reshape(1, cols)
    scale = row_scale(stat2, ts, tr)
    for r in range(nb):
        at = slice(r * LANES, (r + 1) * LANES)
        nbuf[at] = (tbuf[at] * scale[:, r : r + 1]).astype(BF16)
        out_copy(r).start()

    stat_all(stat2, ts, tr).wait_send()
    pltpu.make_async_copy(nbuf, out_ref, xs.at[0]).wait()


def on_device(
    tokens, pre_gain, route_ids, route_weights, gate_weight, up_weight, down_weight, post_gain
):
    tok, cols = tokens.shape
    top = route_ids.shape[1]
    G = lax.axis_size("ep")
    n = lax.axis_size("tp")
    L = n // 2
    cap = 9 * tok * top // (8 * G)
    rows = G * cap
    units = gate_weight.shape[2]
    nb = tok // LANES
    tile = cap
    tiles = tok // min(256, tok)
    vmem = pl.BlockSpec(memory_space=pltpu.VMEM)
    hbm = pl.BlockSpec(memory_space=pl.ANY)
    return pl.pallas_call(
        functools.partial(layer_kernel, L, G, cap, tile),
        out_shape=jax.ShapeDtypeStruct((tok, cols), BF16),
        in_specs=[hbm] + [vmem] * 4 + [hbm] * 3,
        out_specs=hbm,
        scratch_shapes=[
            pltpu.VMEM((L, tok, cols), BF16),
            pltpu.VMEM((tok, cols), BF16),
            pltpu.VMEM((L, G - 1, cap, cols), BF16),
            pltpu.VMEM((2, L, rows, cols), BF16),
            pltpu.VMEM((2, 2, 2 * cols, units), BF16),
            pltpu.VMEM((2, rows, units), F32),
            pltpu.VMEM((2, rows, units), BF16),
            pltpu.VMEM((L, 2 * units, cols), BF16),
            pltpu.VMEM((L, rows, cols), BF16),
            pltpu.VMEM((L + 1, tok, cols), BF16),
            pltpu.VMEM((2, cap, cols), BF16),
            pltpu.VMEM((cap, cols), F32),
            pltpu.VMEM((tok, cols), F32),
            pltpu.VMEM((n, 2 * nb, LANES), F32),
            pltpu.VMEM((n, nb, LANES), F32),
            pltpu.VMEM((G * nb, LANES), jnp.int32),
            pltpu.VMEM((LANES, LANES), jnp.int32),
            pltpu.VMEM((LANES, LANES), F32),
            pltpu.VMEM((LANES, LANES), F32),
            DMA((2, L)), DMA((L,)),
            DMA((L, G)), DMA((L, G)),
            DMA((3,)),
            DMA((L,)), DMA((L, G)),
            DMA((2, 2)),
            DMA((1,)), DMA((1,)), DMA((1,)),
            DMA((G,)), DMA((G,)),
            DMA((L, G)),
            DMA((2,)), DMA((2,)),
            DMA((L,)), DMA((L + 1, tiles)),
            DMA((1,)), DMA((1,)),
            DMA((1,)), DMA((1,)),
            DMA((1,)),
        ],
        compiler_params=pltpu.CompilerParams(
            collective_id=1, has_side_effects=True, vmem_limit_bytes=62 * 2**20
        ),
        name="layer",
    )(
        tokens, pre_gain, post_gain, route_ids.T, route_weights.T,
        gate_weight[0], up_weight[0], down_weight[0],
    )


def solution(mesh):
    placed = (
        P("ep", "tp"),
        P("tp"),
        P("ep", None),
        P("ep", None),
        P("ep", None, "tp"),
        P("ep", None, "tp"),
        P("ep", "tp", None),
        P("tp"),
    )
    return jax.shard_map(
        on_device, mesh=mesh, in_specs=placed, out_specs=P("ep", "tp"), check_vma=False
    )
```
